32 devices in a mesh: grp: 2 (over x), ep: 8 (over z, y), tp: 2 (over core).
Axes of the slice: x: 2, y: 2, z: 4, core: 2. Of those that a mesh axis runs over, the one named last changes fastest.
Arguments:
- tokens: bfloat16 [4096, 2048], P(('grp', 'ep', 'tp')), parts along dimension 0, may hold values from -6 to 6
- norm_gain: float32 [2048], replicated, may hold values from 0.1 to 1.9
- expert_ids: int32 [4096, 2], P(('grp', 'ep', 'tp')), parts along dimension 0, may hold values from 0 to 7, all different within a row; in each aligned block of 128 rows (0 to 127, 128 to 255, ...) at most 64 rows name the same one
- route_weights: float32 [4096, 2], P(('grp', 'ep', 'tp')), parts along dimension 0, may hold values from 0.2 to 1
- gate_proj: bfloat16 [8, 2048, 1536], P('ep', None, 'tp'), may hold values from -0.375 to 0.375
- linear_proj: bfloat16 [8, 2048, 1536], P('ep', None, 'tp'), may hold values from -0.375 to 0.375
- down_proj: bfloat16 [8, 1536, 2048], P('ep', 'tp'), may hold values from -0.01953125 to 0.01953125
Outputs:
- mixed: bfloat16 [4096, 2048], P(('grp', 'ep', 'tp')), parts along dimension 0
The draws below stay inside these ranges and needn't reach their ends.
There are 2 independent parts, one for each index of `grp`. The reference program is written for one: setup_inputs(seed, part) draws one part's arguments, and reference() takes and returns one part's arrays. A program takes and returns all parts, laid end to end along the dimension named above; an argument that names none is the same for every part. Nothing has to cross between parts.
Inputs may be any that keep to these rules, and one draw needn't show every extreme that they name: `expert_ids`: each token names 2 different experts. Among the 128 rows of one device (aligned blocks) no expert is named more than 64 times, a bound that some expert reaches in some blocks.
All inputs are finite; a program needn't handle non-finite values.
Results may differ from the reference program's by a relative error of at most 0.009.
Values may be sent and summed in bfloat16 or wider, within the bound.
A program may use at most 64 MiB of HBM per device.

```python
import math
import jax
import jax.numpy as jnp
import numpy as np
from jax import lax

D = 2048
FF = 1536
TOK_DEV = 128
TOPK = 2
EXPERTS = 8
CAP = 64
TOKENS = 2048
N_EP = 8
N_TP = 2


def block_levels(key, extent, pieces, smallest, top_value):
    gain = 1.0
    for position, shards_of in pieces:
        heights = jax.random.uniform(jax.random.fold_in(jax.random.fold_in(key, 6), position), (shards_of,), jnp.float32, smallest / len(pieces), top_value / len(pieces))
        gain = gain * jnp.repeat(jnp.exp(heights), extent[position] // shards_of).reshape((-1,) + (1,) * (len(extent) - 1 - position))
    return gain


def shared_out(rng, own, number, rows, number_of, top, reach, lean):
    ranking = jax.random.permutation(rng, number_of)
    crowded, ordinary = portions_of(number_of, rows * top, reach, lean, True), portions_of(number_of, rows * top, reach, lean, False)
    places = jnp.arange(number_of)

    def named(tallies, turn):
        used = int((tallies > 0).sum())
        fixed = max(1, used // 4)
        shifted = fixed + (places - fixed + turn * (used - fixed)) % max(1, number_of - fixed)
        return jnp.zeros((number_of,), jnp.int32).at[ranking[jnp.where(places < fixed, places, shifted)]].set(jnp.asarray(tallies, jnp.int32))

    tallies = jnp.where(number % 4 == 0, named(crowded, number // 4), named(ordinary, number - number // 4 - 1))
    mixed = jax.random.permutation(jax.random.fold_in(own, 3), number_of)
    giver, taker = mixed[0:number_of // 2 * 2:2], mixed[1:number_of // 2 * 2:2]
    margin = jnp.minimum(tallies[giver] - 1, reach - tallies[taker]) // 2
    margin = jnp.where((giver == ranking[0]) | (taker == ranking[0]) | (tallies[taker] == 0), 0, jnp.maximum(margin, 0))
    shifted = jax.random.randint(jax.random.fold_in(own, 4), (number_of // 2,), 0, 1 << 20) % (margin + 1)
    tallies = tallies.at[giver].add(-shifted).at[taker].add(shifted)
    labels = jnp.searchsorted(jnp.cumsum(tallies), jnp.arange(rows * top), side="right").astype(jnp.int32)
    grid = labels.reshape(top, rows).T
    grid = grid[jax.random.permutation(jax.random.fold_in(own, 1), rows)]
    turn = jax.random.randint(jax.random.fold_in(own, 2), (rows, 1), 0, top)
    return jnp.take_along_axis(grid, (jnp.arange(top)[None, :] + turn) % top, axis=1)


def portions_of(count, total, reach, skew, full):
    weights = [(1 << 20) // math.isqrt(grade ** skew) + 1 for grade in range(1, count + 1)]
    largest = reach if full else min(reach, max(-(-total // count), total * weights[0] // sum(weights)))
    least = 1 if total - largest >= count - 1 else 0
    counts, surplus = [largest] + [least] * (count - 1), total - largest - least * (count - 1)
    while surplus > 0:
        candidates = [i for i in range(1, count) if counts[i] < largest] or [i for i in range(1, count) if counts[i] < reach]
        mass, remaining = sum([weights[i] for i in candidates]), surplus
        for i in candidates:
            addition = min(reach - counts[i], max(1, remaining * weights[i] // mass), surplus)
            counts[i] = counts[i] + addition
            surplus = surplus - addition
    return np.array(counts)


def normal_values(rng, shape, spread, bound, cuts=(), kind=jnp.bfloat16):
    loudness = block_levels(rng, shape, cuts, -0.22, 0.18) if cuts else 1.0
    drawn = jax.random.normal(rng, shape, jnp.float32) * spread * loudness
    return jnp.minimum(jnp.maximum(drawn, -bound), bound).astype(kind)


def setup_inputs(seed: int = 0, part: int = 0) -> dict:
    keys = jax.random.split(jax.random.key(seed), 8)
    own_keys = jax.random.split(jax.random.fold_in(keys[7], part), 8)
    tokens = normal_values(own_keys[0], (TOKENS, D), 1.0, 6.0, ((0, 16),))
    norm_gain = jnp.clip(1.0 + 0.18 * jax.random.normal(keys[1], (D,), jnp.float32), 0.1, 1.9)
    expert_ids_keys = jax.random.split(jax.random.fold_in(own_keys[2], 1), TOKENS // TOK_DEV)
    expert_ids_turns = jax.random.permutation(jax.random.fold_in(own_keys[2], 3), TOKENS // TOK_DEV)
    expert_ids = jax.vmap(lambda own, number: shared_out(jax.random.fold_in(own_keys[2], 2), own, number, TOK_DEV, EXPERTS, TOPK, CAP, 2))(expert_ids_keys, expert_ids_turns).reshape((TOKENS, TOPK))
    route_weights = jnp.clip(0.2 + 0.8 * jax.random.uniform(own_keys[3], (TOKENS, TOPK), jnp.float32) ** block_levels(own_keys[3], (TOKENS, TOPK), ((0, 16),), -0.2, 0.2), 0.2, 1.0)
    gate_proj = normal_values(keys[4], (EXPERTS, D, FF), (D // 9) ** -0.5, 0.375, ((0, 8), (2, 2)))
    linear_proj = normal_values(keys[5], (EXPERTS, D, FF), (D // 9) ** -0.5, 0.375, ((0, 8), (2, 2)))
    down_proj = normal_values(keys[6], (EXPERTS, FF, D), (FF * 64) ** -0.5, 0.01953125, ((0, 8), (1, 2)))
    return dict(tokens=tokens, norm_gain=norm_gain, expert_ids=expert_ids, route_weights=route_weights, gate_proj=gate_proj, linear_proj=linear_proj, down_proj=down_proj)


def expert_apply(rows, w_gate, w_lin, w_down):
    gate_pre = jnp.dot(rows, w_gate, preferred_element_type=jnp.float32)
    lin_pre = jnp.dot(rows, w_lin, preferred_element_type=jnp.float32)
    glu = jnp.minimum(gate_pre, 7.0)
    lin = jnp.clip(lin_pre, -7.0, 7.0)
    act = (glu * jax.nn.sigmoid(1.702 * glu) * (lin + 1.0)).astype(jnp.bfloat16)
    width = FF // N_TP
    total = jnp.zeros((rows.shape[0], D), jnp.float32)
    for block in range(N_TP):
        partial_value = jnp.dot(act[:, block * width:(block + 1) * width], w_down[block * width:(block + 1) * width], preferred_element_type=jnp.float32).astype(jnp.bfloat16)
        partial_value = lax.optimization_barrier(partial_value)
        total = total + partial_value.astype(jnp.float32)
    return total.astype(jnp.bfloat16)

def reference(tokens, norm_gain, expert_ids, route_weights, gate_proj, linear_proj, down_proj):
    values = tokens.astype(jnp.float32)
    normed = (values * lax.rsqrt(lax.optimization_barrier(jnp.mean(values * values, axis=-1, keepdims=True)) + 1e-06) * norm_gain).astype(jnp.bfloat16)
    flat = expert_ids.reshape(-1).astype(jnp.int32)
    onehot = (flat[:, None] == jnp.arange(EXPERTS, dtype=jnp.int32)[None, :]).astype(jnp.int32)
    slots = lax.optimization_barrier(jnp.sum((jnp.cumsum(onehot, axis=0) - 1) * onehot, axis=1)).astype(jnp.int32)
    per_expert = N_EP * N_TP * CAP
    where = (flat * per_expert + slots).astype(jnp.int32)
    buffer = jnp.zeros((EXPERTS * per_expert, D), jnp.bfloat16).at[where].set(jnp.repeat(normed, TOPK, axis=0))
    buffer = buffer.reshape(EXPERTS, per_expert, D)
    results = lax.map(lambda item: expert_apply(item[0], item[1], item[2], item[3]), (buffer, gate_proj, linear_proj, down_proj))
    picked = results.reshape(EXPERTS * per_expert, D)[where].reshape(TOKENS, TOPK, D).astype(jnp.float32)
    return lax.optimization_barrier(jnp.sum(picked * route_weights[:, :, None], axis=1)).astype(jnp.bfloat16)
```

```python
import functools

import jax
import jax.numpy as jnp
from jax import lax
from jax.experimental import pallas as pl
from jax.experimental.pallas import tpu as pltpu
from jax.sharding import PartitionSpec as P

MESH = pl.DeviceIdType.MESH
LINE = 4
PARTS = 8
BANDS = 4
EARLY = 1

OUTER_PLAN = (
    0, 1, 2, 3, 4, 5, 6, 7, 500, 100, 10, 101, 510, 102, 11, 103, 104, 12, 105, 106,
    13, 107, 110, 200, 14, 111, 112, 201, 15, 113, 202, 300, 16, 114, 301, 302, 17, 115, 400, 303,
    401, 402, 30, 530, 116, 403, 117, 20, 520, 210, 21, 211, 212, 22, 120, 310, 311, 23, 121, 312,
    313, 24, 130, 410, 411, 122, 412, 413, 25, 123, 124, 26, 610, 611, 27, 612, 613, 31, 614, 615,
    32, 616, 617, 33, 125, 126, 34, 127, 131, 35, 220, 221, 36, 222, 37, 320, 321, 322, 323, 420,
    132, 133, 134, 135, 136, 421, 137, 422, 423, 800, 801, 802, 803, 804, 805, 806, 807, 230, 620, 231,
    621, 232, 622, 623, 330, 624, 331, 625, 332, 430, 626, 627, 431, 333, 432, 433, 600, 630, 601, 631,
    632, 602, 633, 634, 603, 635, 636, 604, 637, 605, 606, 607,
)
INNER_PLAN = (
    0, 1, 2, 3, 4, 5, 6, 7, 500, 100, 10, 510, 30, 530, 101, 102, 11, 103, 104, 12,
    105, 20, 520, 106, 13, 107, 21, 110, 200, 22, 130, 14, 111, 201, 23, 15, 112, 120, 202, 16,
    113, 300, 121, 301, 24, 17, 701, 702, 703, 704, 705, 706, 707, 122, 302, 114, 400, 303, 25, 123,
    401, 402, 115, 26, 403, 116, 124, 27, 117, 125, 31, 210, 126, 211, 127, 32, 212, 131, 33, 220,
    221, 222, 132, 133, 34, 35, 320, 321, 322, 36, 323, 420, 421, 134, 310, 37, 422, 135, 311, 423,
    800, 801, 802, 803, 804, 805, 806, 807, 312, 136, 313, 410, 411, 412, 413, 137, 230, 231, 232, 330,
    331, 332, 333, 430, 431, 432, 433, 620, 621, 622, 610, 623, 611, 624, 612, 625, 613, 626, 614, 627,
    615, 630, 616, 631, 617, 632, 600, 633, 601, 634, 602, 635, 603, 636, 604, 637, 605, 606, 607,
)


def shards(tokens, norm_gain, expert_ids, route_weights, gate_proj, linear_proj, down_proj):
    tok_count, width = tokens.shape
    picks = expert_ids.shape[1]
    experts = lax.axis_size("ep")
    capacity = 2 * tok_count * picks // experts
    values = tokens.astype(jnp.float32)
    normed = (
        values * lax.rsqrt(jnp.mean(values * values, axis=-1, keepdims=True) + 1e-06) * norm_gain
    ).astype(jnp.bfloat16)
    flat = expert_ids.reshape(-1)
    onehot = (flat[:, None] == jnp.arange(experts, dtype=jnp.int32)[None, :]).astype(jnp.int32)
    slots = jnp.sum((jnp.cumsum(onehot, axis=0) - 1) * onehot, axis=1)
    where = flat * capacity + slots
    buffer = (
        jnp.zeros((experts * capacity, width), jnp.bfloat16)
        .at[where]
        .set(jnp.repeat(normed, picks, axis=0))
    )
    arrived = lax.all_to_all(buffer, "ep", split_axis=0, concat_axis=0, tiled=True)
    rows = lax.all_gather(arrived, "tp", axis=0, tiled=True)
    gate_pre = jnp.dot(rows, gate_proj[0], preferred_element_type=jnp.float32)
    lin_pre = jnp.dot(rows, linear_proj[0], preferred_element_type=jnp.float32)
    glu = jnp.minimum(gate_pre, 7.0)
    lin = jnp.clip(lin_pre, -7.0, 7.0)
    hidden = (glu * jax.nn.sigmoid(1.702 * glu) * (lin + 1.0)).astype(jnp.bfloat16)
    rows = hidden
    summed = lax.psum_scatter(
        jnp.dot(rows, down_proj[0], preferred_element_type=jnp.float32).astype(jnp.bfloat16),
        "tp",
        scatter_dimension=0,
        tiled=True,
    )
    returned = lax.all_to_all(summed, "ep", split_axis=0, concat_axis=0, tiled=True)
    picked = returned[where].reshape(tok_count, picks, width).astype(jnp.float32)
    return jnp.sum(picked * route_weights[:, :, None], axis=1).astype(jnp.bfloat16)


def kernel(
    ids_ref, weights_ref, gain_ref, tokens_ref, gate_hbm, linear_hbm, down_hbm, out_ref,
    gate, linear, down, tok, meta, pick, spread, shares, rows, cross, hidden, part, part_in, done,
    back_in, ret_in, ret_out,
    load_sem, tok_send, tok_recv, meta_send, meta_recv, cross_send, cross_recv, pair_send, pair_recv,
    part_send, part_recv, back_send, back_recv, ret_send, ret_recv,
):
    ep, core = lax.axis_index("ep"), lax.axis_index("tp")
    z, y = ep // 2, ep % 2
    experts = 2 * LINE
    tok_count, width = tokens_ref.shape
    capacity = rows.shape[3]
    ff = gate.shape[1]
    cols = [pl.ds(i * (width // PARTS), width // PARTS) for i in range(PARTS)]
    bands = [pl.ds(i * (width // BANDS), width // BANDS) for i in range(BANDS)]
    units = [pl.ds(i * 256, 256) for i in range(ff // 256)]
    here, there = z * 2 + y, z * 2 + 1 - y
    at_y = {"ep": there}
    at_core = {"tp": 1 - core}
    outwards = jnp.where(z < LINE // 2, -1, 1)
    outer = (z == 0) | (z == LINE - 1)

    def at_z(other):
        return {"ep": other * 2 + y}

    def remote(source, target, send, recv, device):
        return pltpu.make_async_remote_copy(
            src_ref=source, dst_ref=target, send_sem=send, recv_sem=recv,
            device_id=device, device_id_type=MESH,
        )

    loads = [
        pltpu.make_async_copy(source, target, load_sem.at[i])
        for i, (source, target) in enumerate(((gate_hbm, gate), (linear_hbm, linear), (down_hbm, down)))
    ]
    for load in loads:
        load.start()
    barrier = pltpu.get_barrier_semaphore()
    for step in range(1, LINE):
        pl.semaphore_signal(barrier, 1, device_id=at_z(lax.rem(z + step, LINE)), device_id_type=MESH)
    pl.semaphore_signal(barrier, 1, device_id=at_y, device_id_type=MESH)
    pl.semaphore_signal(barrier, 1, device_id=at_core, device_id_type=MESH)

    def normalize(i, _):
        span = pl.ds(pl.multiple_of(i * 32, 32), 32)
        values = tokens_ref[span, :].astype(jnp.float32)
        scale = lax.rsqrt(jnp.mean(values * values, axis=-1, keepdims=True) + 1e-06)
        tok[z, span, :] = (values * scale * gain_ref[...]).astype(jnp.bfloat16)
        return 0

    lax.fori_loop(0, tok_count // 32, normalize, 0)
    names = lax.broadcasted_iota(jnp.int32, (experts, tok_count), 0)
    share = jnp.zeros((experts, tok_count), jnp.float32)
    chosen = jnp.zeros((experts, tok_count), jnp.float32)
    for choice in range(ids_ref.shape[0]):
        same = ids_ref[choice : choice + 1, :] == names
        share = share + jnp.where(same, weights_ref[choice : choice + 1, :], 0.0)
        chosen = chosen + jnp.where(same, 1.0, 0.0)
    first = lax.broadcasted_iota(jnp.int32, (tok_count, tok_count), 0)
    second = lax.broadcasted_iota(jnp.int32, (tok_count, tok_count), 1)
    before = jnp.where(first < second, 1.0, 0.0).astype(jnp.bfloat16)
    slots = jnp.dot(chosen.astype(jnp.bfloat16), before, preferred_element_type=jnp.float32)
    meta[z, 0:experts, :] = jnp.where(chosen > 0.5, slots, -1.0)
    meta[z, experts : 2 * experts, :] = share
    pl.semaphore_wait(barrier, LINE + 1)

    def meta_copy(step):
        return remote(
            meta.at[z], meta.at[z], meta_send.at[step], meta_recv.at[z], at_z(lax.rem(z + step, LINE))
        )

    def meta_arrival(source):
        return remote(
            meta.at[source], meta.at[source], meta_send.at[0], meta_recv.at[source],
            at_z(lax.rem(z + 1, LINE)),
        )

    def hop(source, i, way):
        block = tok.at[source, :, cols[i]]
        other = z + outwards if way else z - outwards
        return remote(
            block, block, tok_send.at[source, i, way], tok_recv.at[source, i], at_z(other)
        )

    def cross_copy(source, i):
        return remote(
            cross.at[source, :, cols[i]], rows.at[source, core, y, :, cols[i]],
            cross_send.at[source, i], cross_recv.at[source, i], at_y,
        )

    def cross_arrival(source, i):
        return remote(
            cross.at[source, :, cols[i]], rows.at[source, core, 1 - y, :, cols[i]],
            cross_send.at[source, i], cross_recv.at[source, i], at_y,
        )

    def pair_move(source, owner, column, i):
        block = rows.at[source, owner, column, :, cols[i]]
        return remote(block, block, pair_send.at[source, column, i], pair_recv.at[source, column, i], at_core)

    def part_copy(source, i):
        return remote(
            part.at[source, 1 - core, :, :, bands[i]], part_in.at[source, :, :, bands[i]],
            part_send.at[source, i], part_recv.at[source, i], at_core,
        )

    def back_copy(source, i):
        return remote(
            done.at[source, 1 - y, :, cols[i]], back_in.at[source, :, cols[i]],
            back_send.at[source, i], back_recv.at[source, i], at_y,
        )

    def ret_copy(source, i, way):
        step = outwards if way else -outwards
        side = jnp.where(step > 0, 0, 1)
        return remote(
            ret_out.at[source, :, cols[i]], ret_in.at[side, source, :, cols[i]],
            ret_send.at[source, i], ret_recv.at[side, source, i], at_z(z + step),
        )

    def ret_arrival(source, i, way):
        step = -outwards if way else outwards
        side = jnp.where(step > 0, 0, 1)
        return side, remote(
            ret_out.at[source, :, cols[i]], ret_in.at[side, source, :, cols[i]],
            ret_send.at[source, i], ret_recv.at[side, source, i], at_z(z - step),
        )

    def run(plan, at_end):
        if at_end:
            order = [z, z - outwards, z - 3 * outwards, z - 2 * outwards]
            passes = [(0,), (), (), ()]
            leaves = [None, 0, 0, 0]
            comes = [(0,), (), (), ()]
        else:
            order = [z, z + outwards, z - 2 * outwards, z - outwards]
            passes = [(1, 0), (0,), (1,), (1,)]
            leaves = [None, 1, 0, 0]
            comes = [(0, 1), (0,), (1,), (1,)]
        waited = [False, False]

        def send_rows(t, i):
            source = order[t]
            if t:
                hop(source, i, 0).wait_recv()
                for way in passes[t]:
                    hop(source, i, way).start()
            if i == 0:
                if t:
                    meta_arrival(source).wait_recv()
                place = lax.broadcasted_iota(jnp.int32, (capacity, tok_count), 0).astype(jnp.float32)
                for half, expert in enumerate((there, here)):
                    pick[t, half * capacity : (half + 1) * capacity, :] = (
                        meta[source, pl.ds(expert, 1), :] == place
                    ).astype(jnp.bfloat16)
            both = jnp.dot(
                pick[t], tok[source, :, cols[i]], preferred_element_type=jnp.float32
            ).astype(jnp.bfloat16)
            cross[source, :, cols[i]] = both[:capacity]
            cross_copy(source, i).start()
            rows[source, core, y, :, cols[i]] = both[capacity:]
            pair_move(source, core, y, i).start()

        def share_rows(t, i):
            source = order[t]
            cross_arrival(source, i).wait_recv()
            pair_move(source, core, 1 - y, i).start()

        def up(t, i):
            source = order[t]
            if i == 0:
                for column in range(2):
                    for j in range(PARTS):
                        pair_move(source, 1 - core, column, j).wait_recv()
                if not waited[0]:
                    waited[0] = True
                    loads[0].wait()
                    loads[1].wait()
            block = rows[source].reshape(4 * capacity, width)
            glu = jnp.minimum(jnp.dot(block, gate[:, units[i]], preferred_element_type=jnp.float32), 7.0)
            lin = jnp.clip(jnp.dot(block, linear[:, units[i]], preferred_element_type=jnp.float32), -7.0, 7.0)
            hidden[t, :, units[i]] = (glu * jax.nn.sigmoid(1.702 * glu) * (lin + 1.0)).astype(jnp.bfloat16)

        def out(t, i):
            source = order[t]
            if not waited[1]:
                waited[1] = True
                loads[2].wait()
            part[source, :, :, :, bands[i]] = (
                jnp.dot(hidden[t], down[:, bands[i]], preferred_element_type=jnp.float32)
                .astype(jnp.bfloat16)
                .reshape(2, 2, capacity, width // BANDS)
            )
            part_copy(source, i).start()

        def add(t, i):
            source = order[t]
            part_copy(source, i).wait_recv()
            done[source, :, :, bands[i]] = (
                part[source, core, :, :, bands[i]].astype(jnp.float32)
                + part_in[source, :, :, bands[i]].astype(jnp.float32)
            ).astype(jnp.bfloat16)
            if t:
                for j in range(i * PARTS // BANDS, (i + 1) * PARTS // BANDS):
                    back_copy(source, j).start()

        def turn(t, i):
            source = order[t]
            eye = lax.broadcasted_iota(jnp.int32, (tok_count, tok_count), 0) == lax.broadcasted_iota(
                jnp.int32, (tok_count, tok_count), 1
            )
            lane = lax.broadcasted_iota(jnp.int32, (tok_count, capacity), 1).astype(jnp.float32)

            def upright(row):
                return jnp.sum(jnp.where(eye, meta[source, pl.ds(row, 1), :], 0.0), axis=1, keepdims=True)

            for half, expert in enumerate((here, there)):
                spread[t, half] = (upright(expert) == lane).astype(jnp.bfloat16)
                shares[t, half] = jnp.broadcast_to(upright(experts + expert), (tok_count, 128))

        def merge(t, i):
            source = order[t]
            back_copy(source, i).wait_recv()
            total = None
            for half, block in enumerate((done[source, y, :, cols[i]], back_in[source, :, cols[i]])):
                scale = jnp.concatenate([shares[t, half]] * (width // PARTS // 128), axis=1)
                term = scale * jnp.dot(spread[t, half], block, preferred_element_type=jnp.float32)
                total = term if total is None else total + term
            for way in comes[t]:
                side, arrival = ret_arrival(source, i, way)
                arrival.wait_recv()
                total = total + ret_in[side, source, :, cols[i]].astype(jnp.float32)
            if t:
                ret_out[source, :, cols[i]] = total.astype(jnp.bfloat16)
                ret_copy(source, i, leaves[t]).start()
            else:
                out_ref[:, cols[i]] = total.astype(jnp.bfloat16)

        def late(t, i):
            hop(z, i, 0).start()

        def own_back(t, i):
            back_copy(z, i).start()

        for step in range(1, LINE):
            meta_copy(step).start()
        for way in passes[0]:
            for i in range(PARTS if at_end or way else EARLY):
                hop(z, i, way).start()
        stages = (send_rows, share_rows, up, out, add, turn, merge, late, own_back)
        for number in plan:
            stages[number // 100](number // 10 % 10, number % 10)
        for step in range(1, LINE):
            meta_copy(step).wait_send()
        for t in range(LINE):
            source = order[t]
            for i in range(PARTS):
                for way in passes[t]:
                    hop(source, i, way).wait_send()
                cross_copy(source, i).wait_send()
                for column in range(2):
                    pair_move(source, core, column, i).wait_send()
                back_copy(source, i).wait_send()
                if t:
                    ret_copy(source, i, leaves[t]).wait_send()
            for i in range(BANDS):
                part_copy(source, i).wait_send()

    pl.when(outer)(lambda: run(OUTER_PLAN, True))
    pl.when(jnp.logical_not(outer))(lambda: run(INNER_PLAN, False))


def fused(tokens, norm_gain, expert_ids, route_weights, gate_proj, linear_proj, down_proj):
    tok_count, width = tokens.shape
    picks = expert_ids.shape[1]
    experts = 2 * LINE
    capacity = 2 * tok_count * picks // experts
    ff = gate_proj.shape[2]
    wide, dma = jnp.bfloat16, pltpu.SemaphoreType.DMA
    inside, outside = pl.BlockSpec(memory_space=pltpu.VMEM), pl.BlockSpec(memory_space=pl.ANY)
    return pl.pallas_call(
        kernel,
        out_shape=jax.ShapeDtypeStruct((tok_count, width), wide),
        in_specs=[inside] * 4 + [outside] * 3,
        out_specs=inside,
        scratch_shapes=[
            pltpu.VMEM((width, ff), wide),
            pltpu.VMEM((width, ff), wide),
            pltpu.VMEM((ff, width), wide),
            pltpu.VMEM((LINE, tok_count, width), wide),
            pltpu.VMEM((LINE, 2 * experts, tok_count), jnp.float32),
            pltpu.VMEM((LINE, 2 * capacity, tok_count), wide),
            pltpu.VMEM((LINE, 2, tok_count, capacity), wide),
            pltpu.VMEM((LINE, 2, tok_count, 128), jnp.float32),
            pltpu.VMEM((LINE, 2, 2, capacity, width), wide),
            pltpu.VMEM((LINE, capacity, width), wide),
            pltpu.VMEM((LINE, 4 * capacity, ff), wide),
            pltpu.VMEM((LINE, 2, 2, capacity, width), wide),
            pltpu.VMEM((LINE, 2, capacity, width), wide),
            pltpu.VMEM((LINE, 2, capacity, width), wide),
            pltpu.VMEM((LINE, capacity, width), wide),
            pltpu.VMEM((2, LINE, tok_count, width), wide),
            pltpu.VMEM((LINE, tok_count, width), wide),
            dma((3,)),
            dma((LINE, PARTS, 2)), dma((LINE, PARTS)),
            dma((LINE,)), dma((LINE,)),
            dma((LINE, PARTS)), dma((LINE, PARTS)),
            dma((LINE, 2, PARTS)), dma((LINE, 2, PARTS)),
            dma((LINE, BANDS)), dma((LINE, BANDS)),
            dma((LINE, PARTS)), dma((LINE, PARTS)),
            dma((LINE, PARTS)), dma((2, LINE, PARTS)),
        ],
        compiler_params=pltpu.CompilerParams(
            collective_id=0, has_side_effects=True, vmem_limit_bytes=60 * 1024 * 1024
        ),
        name="experts",
    )(
        expert_ids.T, route_weights.T, norm_gain.reshape(1, width), tokens,
        gate_proj[0], linear_proj[0], down_proj[0],
    )


def solution(mesh):
    placed = (
        P(("grp", "ep", "tp"), None),
        P(),
        P(("grp", "ep", "tp"), None),
        P(("grp", "ep", "tp"), None),
        P("ep", None, "tp"),
        P("ep", None, "tp"),
        P("ep", "tp", None),
    )
    along = [device.coords[2] for device in mesh.devices[0, :, 0]]
    planned = along == [index // 2 for index in range(2 * LINE)] and mesh.shape["tp"] == 2
    return jax.shard_map(
        fused if planned else shards,
        mesh=mesh,
        in_specs=placed,
        out_specs=P(("grp", "ep", "tp"), None),
        check_vma=False,
    )
```

```python
import functools

import jax
import jax.numpy as jnp
from jax import lax
from jax.experimental import pallas as pl
from jax.experimental.pallas import tpu as pltpu
from jax.sharding import PartitionSpec as P

MESH = pl.DeviceIdType.MESH
LINE = 4
PARTS = 4
BANDS = 2

OUTER_TURNS = (0, -1, -3, -2)
INNER_TURNS = (0, 1, -2, -1)
OUTER_PLAN = (
    7000, 7001, 7002, 7003, 7010, 7011, 7012, 7013, 0, 1, 2, 3, 10, 11, 12, 13,
    5000, 5010, 1000, 100, 5100, 1001, 1002, 101, 1003, 1010, 102, 1011, 1012, 103, 1013, 1100,
    300, 5300, 1101, 1102, 301, 1103, 1300, 302, 2100, 303, 1301, 3100, 310, 1302, 5310, 4100,
    4101, 311, 1303, 2300, 312, 313, 6100, 6101, 3300, 200, 6102, 6103, 201, 4300, 4301, 5200,
    1310, 1311, 1312, 1313, 202, 1200, 2310, 203, 6300, 6301, 1201, 3310, 210, 4310, 211, 4311,
    6302, 6303, 1202, 1203, 5210, 212, 2200, 213, 6310, 6311, 110, 1210, 1211, 3200, 111, 4200,
    6312, 4201, 6313, 1212, 5110, 112, 1213, 1110, 113, 2210, 6200, 6201, 3210, 6202, 6203, 4210,
    4211, 1111, 1112, 1113, 2110, 6210, 6211, 3110, 6212, 4110, 6213, 4111, 2000, 6110, 3000, 6111,
    6112, 6113, 4000, 4001, 9000, 9001, 9002, 9003, 4010, 9010, 9011, 4011, 9012, 9013, 6000, 6001,
    6002, 6003, 6010, 6011, 6012, 6013,
)
INNER_PLAN = (
    7000, 8000, 7001, 8001, 7002, 8002, 7003, 0, 5000, 1, 2, 3, 10, 5010, 11, 12,
    13, 8003, 8010, 8011, 8012, 8013, 1000, 300, 5300, 1001, 100, 5100, 1002, 301, 101, 1003,
    1010, 302, 102, 1011, 1012, 303, 103, 1013, 1300, 310, 5310, 1100, 110, 5110, 1301, 311,
    111, 1101, 1302, 312, 112, 1102, 1303, 313, 113, 1103, 2300, 200, 2100, 201, 202, 3100,
    203, 4100, 5200, 4101, 1110, 1111, 1112, 1113, 3300, 2110, 4300, 4301, 210, 5210, 211, 212,
    1200, 1201, 1202, 1203, 1310, 1311, 1312, 1313, 3110, 213, 7010, 7011, 7012, 7013, 4110, 2310,
    4111, 3310, 6300, 4310, 2200, 6301, 4311, 3200, 6302, 4200, 6303, 4201, 1210, 1211, 1212, 1213,
    2000, 6310, 6311, 3000, 6312, 4000, 4001, 2210, 6313, 3210, 6200, 4210, 4010, 4211, 9000, 9001,
    9002, 9003, 6201, 9010, 9011, 4011, 9012, 9013, 6202, 6100, 6203, 6101, 6210, 6000, 6102, 6211,
    6001, 6002, 6103, 6212, 6003, 6110, 6213, 6111, 6010, 6112, 6011, 6113, 6012, 6013,
)


def shards(tokens, norm_gain, expert_ids, route_weights, gate_proj, linear_proj, down_proj):
    tok_count, width = tokens.shape
    picks = expert_ids.shape[1]
    experts = lax.axis_size("ep")
    capacity = 2 * tok_count * picks // experts
    values = tokens.astype(jnp.float32)
    normed = (
        values * lax.rsqrt(jnp.mean(values * values, axis=-1, keepdims=True) + 1e-06) * norm_gain
    ).astype(jnp.bfloat16)
    flat = expert_ids.reshape(-1)
    onehot = (flat[:, None] == jnp.arange(experts, dtype=jnp.int32)[None, :]).astype(jnp.int32)
    slots = jnp.sum((jnp.cumsum(onehot, axis=0) - 1) * onehot, axis=1)
    where = flat * capacity + slots
    buffer = (
        jnp.zeros((experts * capacity, width), jnp.bfloat16)
        .at[where]
        .set(jnp.repeat(normed, picks, axis=0))
    )
    arrived = lax.all_to_all(buffer, "ep", split_axis=0, concat_axis=0, tiled=True)
    rows = lax.all_gather(arrived, "tp", axis=0, tiled=True)
    gate_pre = jnp.dot(rows, gate_proj[0], preferred_element_type=jnp.float32)
    lin_pre = jnp.dot(rows, linear_proj[0], preferred_element_type=jnp.float32)
    glu = jnp.minimum(gate_pre, 7.0)
    lin = jnp.clip(lin_pre, -7.0, 7.0)
    hidden = (glu * jax.nn.sigmoid(1.702 * glu) * (lin + 1.0)).astype(jnp.bfloat16)
    rows = hidden
    summed = lax.psum_scatter(
        jnp.dot(rows, down_proj[0], preferred_element_type=jnp.float32).astype(jnp.bfloat16),
        "tp",
        scatter_dimension=0,
        tiled=True,
    )
    returned = lax.all_to_all(summed, "ep", split_axis=0, concat_axis=0, tiled=True)
    picked = returned[where].reshape(tok_count, picks, width).astype(jnp.float32)
    return jnp.sum(picked * route_weights[:, :, None], axis=1).astype(jnp.bfloat16)


def kernel(
    ids_ref, weights_ref, gain_ref, tokens_hbm, gate_hbm, linear_hbm, down_hbm, out_ref,
    tokens_ref, gate, linear, down, mate, tok, meta, pick, spread, shares, rows, cross, hidden, part, part_in, done,
    back_in, ret_in, ret_out, last, last_in,
    load_sem, mate_send, mate_recv, tok_send, tok_recv, meta_send, meta_recv, cross_send, cross_recv,
    pair_send, pair_recv, part_send, part_recv, back_send, back_recv, ret_send, ret_recv,
    last_send, last_recv,
):
    ep, core = lax.axis_index("ep"), lax.axis_index("tp")
    z, y = ep // 2, ep % 2
    experts = 2 * LINE
    tok_count, width = tokens_hbm.shape
    half = width // 2
    capacity = cross.shape[2]
    ff = gate.shape[1]
    step_cols, step_band, unit = half // PARTS, half // BANDS, 256
    cols = [pl.ds(i * step_cols, step_cols) for i in range(PARTS)]
    here, there = z * 2 + y, z * 2 + 1 - y
    mine = pl.ds(pl.multiple_of(core * half, half), half)
    other = pl.ds(pl.multiple_of((1 - core) * half, half), half)
    at_y = {"ep": there}
    at_core = {"tp": 1 - core}
    outwards = jnp.where(z < LINE // 2, -1, 1)
    outer = (z == 0) | (z == LINE - 1)

    def at_z(other):
        return {"ep": other * 2 + y}

    def remote(source, target, send, recv, device):
        return pltpu.make_async_remote_copy(
            src_ref=source, dst_ref=target, send_sem=send, recv_sem=recv,
            device_id=device, device_id_type=MESH,
        )

    peers = [at_core] + [
        {"ep": lax.rem(z + step, LINE) * 2 + y, "tp": tp} for step in range(1, LINE) for tp in range(2)
    ]
    loads = [
        pltpu.make_async_copy(source, target, load_sem.at[i])
        for i, (source, target) in enumerate(((gate_hbm, gate), (linear_hbm, linear), (down_hbm, down)))
    ]
    fetch = pltpu.make_async_copy(tokens_hbm, tokens_ref, load_sem.at[3])
    fetch.start()
    barrier = pltpu.get_barrier_semaphore()
    for device in peers + [at_y]:
        pl.semaphore_signal(barrier, 1, device_id=device, device_id_type=MESH)

    def normalize(i, _):
        span = pl.ds(pl.multiple_of(i * 32, 32), 32)
        values = tokens_ref[span, :].astype(jnp.float32)
        scale = lax.rsqrt(jnp.mean(values * values, axis=-1, keepdims=True) + 1e-06)
        mate[span, :] = (tokens_ref[span, other].astype(jnp.float32) * scale * gain_ref[:, other]).astype(
            jnp.bfloat16
        )
        tok[z, core, span, :] = (tokens_ref[span, mine].astype(jnp.float32) * scale * gain_ref[:, mine]).astype(
            jnp.bfloat16
        )
        return 0

    fetch.wait()
    for load in loads:
        load.start()
    lax.fori_loop(0, tok_count // 32, normalize, 0)
    pl.semaphore_wait(barrier, len(peers) + 1)
    mate_copy = remote(mate, tok.at[z, core], mate_send.at[0], mate_recv.at[0], at_core)
    mate_copy.start()
    names = lax.broadcasted_iota(jnp.int32, (experts, tok_count), 0)
    share = jnp.zeros((experts, tok_count), jnp.float32)
    chosen = jnp.zeros((experts, tok_count), jnp.float32)
    for choice in range(ids_ref.shape[0]):
        same = ids_ref[choice : choice + 1, :] == names
        share = share + jnp.where(same, weights_ref[choice : choice + 1, :], 0.0)
        chosen = chosen + jnp.where(same, 1.0, 0.0)
    first = lax.broadcasted_iota(jnp.int32, (tok_count, tok_count), 0)
    second = lax.broadcasted_iota(jnp.int32, (tok_count, tok_count), 1)
    before = jnp.where(first < second, 1.0, 0.0).astype(jnp.bfloat16)
    slots = jnp.dot(chosen.astype(jnp.bfloat16), before, preferred_element_type=jnp.float32)
    meta[z, core, 0:experts, :] = jnp.where(chosen > 0.5, slots, -1.0)
    meta[z, core, experts : 2 * experts, :] = share

    def meta_copy(k):
        block = meta.at[z, core]
        return remote(block, block, meta_send.at[k], meta_recv.at[z, core], peers[k])

    def meta_arrival(source, h):
        block = meta.at[source, h]
        return remote(block, block, meta_send.at[0], meta_recv.at[source, h], at_core)

    def hop(source, h, i, way):
        block = tok.at[source, h, :, cols[i]]
        target = z + outwards if way else z - outwards
        return remote(
            block, block, tok_send.at[source, h, i, way], tok_recv.at[source, h, i], at_z(target)
        )

    def cross_copy(source, h, i):
        return remote(
            cross.at[source, h, :, cols[i]], rows.at[source, h, core, y, :, cols[i]],
            cross_send.at[source, h, i], cross_recv.at[source, h, i], at_y,
        )

    def cross_arrival(source, h, i):
        return remote(
            cross.at[source, h, :, cols[i]], rows.at[source, h, core, 1 - y, :, cols[i]],
            cross_send.at[source, h, i], cross_recv.at[source, h, i], at_y,
        )

    def pair_move(source, h, owner, column, i):
        block = rows.at[source, h, owner, column, :, cols[i]]
        return remote(
            block, block, pair_send.at[source, h, column, i], pair_recv.at[source, h, column, i], at_core
        )

    def part_copy(source, h, i):
        band = pl.ds(i * step_band, step_band) if isinstance(i, int) else pl.ds(
            pl.multiple_of(i * step_band, step_band), step_band
        )
        return remote(
            part.at[source, h, 1 - core, :, :, band], part_in.at[source, h, :, :, band],
            part_send.at[source, h, i], part_recv.at[source, h, i], at_core,
        )

    def back_copy(source, h, i):
        return remote(
            done.at[source, h, 1 - y, :, cols[i]], back_in.at[source, h, :, cols[i]],
            back_send.at[source, h, i], back_recv.at[source, h, i], at_y,
        )

    def ret_copy(source, h, i, way):
        step = outwards if way else -outwards
        side = jnp.where(step > 0, 0, 1)
        return remote(
            ret_out.at[source, h, :, cols[i]], ret_in.at[side, source, h, :, cols[i]],
            ret_send.at[source, h, i], ret_recv.at[side, source, h, i], at_z(z + step),
        )

    def ret_arrival(source, h, i, way):
        step = -outwards if way else outwards
        side = jnp.where(step > 0, 0, 1)
        return side, remote(
            ret_out.at[source, h, :, cols[i]], ret_in.at[side, source, h, :, cols[i]],
            ret_send.at[source, h, i], ret_recv.at[side, source, h, i], at_z(z - step),
        )

    def last_copy(h, i):
        return remote(
            last.at[h, :, cols[i]], last_in.at[:, cols[i]], last_send.at[i], last_recv.at[i], at_core
        )

    def run(plan, turns, at_end):
        order = [z + outwards * turn for turn in turns]
        if at_end:
            passes = [(0,), (), (), ()]
            comes = [(0,), (), (), ()]
        else:
            passes = [(1, 0)] + [(0,) if turn > 0 else (1,) for turn in turns[1:]]
            comes = [(0, 1)] + [(0,) if turn > 0 else (1,) for turn in turns[1:]]
        leaves = [None] + [1 if turn > 0 else 0 for turn in turns[1:]]
        waited = [False, False]

        def send_rows(t, h, i):
            source = order[t]
            if t:
                hop(source, h, i, 0).wait_recv()
                for way in passes[t]:
                    hop(source, h, i, way).start()
            if i == 0:
                if t:
                    meta_arrival(source, h).wait_recv()
                place = lax.broadcasted_iota(jnp.int32, (capacity, tok_count), 0).astype(jnp.float32)
                for k, expert in enumerate((there, here)):
                    pick[t, h, k * capacity : (k + 1) * capacity, :] = (
                        meta[source, h, pl.ds(expert, 1), :] == place
                    ).astype(jnp.bfloat16)
            both = jnp.dot(
                pick[t, h], tok[source, h, :, cols[i]], preferred_element_type=jnp.float32
            ).astype(jnp.bfloat16)
            cross[source, h, :, cols[i]] = both[:capacity]
            cross_copy(source, h, i).start()
            rows[source, h, core, y, :, cols[i]] = both[capacity:]
            pair_move(source, h, core, y, i).start()

        def share_rows(t, h, i):
            source = order[t]
            cross_arrival(source, h, i).wait_recv()
            pair_move(source, h, core, 1 - y, i).start()

        def up(t, h, i):
            source = order[t]
            blocks = range(h, h + 1) if t else range(2)
            for block in blocks:
                for column in range(2):
                    for j in range(PARTS):
                        pair_move(source, block, 1 - core, column, j).wait_recv()
            if not waited[0]:
                waited[0] = True
                loads[0].wait()
                loads[1].wait()
            span_h = slice(blocks[0], blocks[-1] + 1)

            def units(j, _):
                span = pl.ds(pl.multiple_of(j * unit, unit), unit)
                low = rows[source, span_h, 0].reshape(len(blocks) * 2 * capacity, half)
                high = rows[source, span_h, 1].reshape(len(blocks) * 2 * capacity, half)

                def through(matrix):
                    return jnp.dot(low, matrix[:half, span], preferred_element_type=jnp.float32) + jnp.dot(
                        high, matrix[half:, span], preferred_element_type=jnp.float32
                    )

                glu = jnp.minimum(through(gate), 7.0)
                lin = jnp.clip(through(linear), -7.0, 7.0)
                hidden[t, span_h, :, span] = (
                    (glu * jax.nn.sigmoid(1.702 * glu) * (lin + 1.0))
                    .astype(jnp.bfloat16)
                    .reshape(len(blocks), 2 * capacity, unit)
                )
                return 0

            lax.fori_loop(0, ff // unit, units, 0)

        def out(t, h, i):
            source = order[t]
            blocks = range(h, h + 1) if t else range(2)
            span_h = slice(blocks[0], blocks[-1] + 1)
            if not waited[1]:
                waited[1] = True
                loads[2].wait()

            def bands(side, send):
                def go(j, _):
                    start = side * half + j * step_band
                    span = pl.ds(pl.multiple_of(start, step_band), step_band)
                    inputs = hidden[t, span_h].reshape(len(blocks) * 2 * capacity, ff)
                    part[source, span_h, side, :, :, pl.ds(pl.multiple_of(j * step_band, step_band), step_band)] = (
                        jnp.dot(inputs, down[:, span], preferred_element_type=jnp.float32)
                        .astype(jnp.bfloat16)
                        .reshape(len(blocks), 2, capacity, step_band)
                    )
                    if send:
                        for block in blocks:
                            part_copy(source, block, j).start()
                    return 0

                lax.fori_loop(0, BANDS, go, 0)

            bands(1 - core, True)
            bands(core, False)

        def add(t, h, i):
            source = order[t]
            part_copy(source, h, i).wait_recv()
            band = pl.ds(i * step_band, step_band)
            done[source, h, :, :, band] = (
                part[source, h, core, :, :, band].astype(jnp.float32)
                + part_in[source, h, :, :, band].astype(jnp.float32)
            ).astype(jnp.bfloat16)
            if t:
                for j in range(i * PARTS // BANDS, (i + 1) * PARTS // BANDS):
                    back_copy(source, h, j).start()

        def turn_over(t, h, i):
            source = order[t]
            eye = lax.broadcasted_iota(jnp.int32, (tok_count, tok_count), 0) == lax.broadcasted_iota(
                jnp.int32, (tok_count, tok_count), 1
            )
            lane = lax.broadcasted_iota(jnp.int32, (tok_count, capacity), 1).astype(jnp.float32)

            def upright(row):
                return jnp.sum(jnp.where(eye, meta[source, h, pl.ds(row, 1), :], 0.0), axis=1, keepdims=True)

            for k, expert in enumerate((here, there)):
                spread[t, h, k] = (upright(expert) == lane).astype(jnp.bfloat16)
                shares[t, h, k] = jnp.broadcast_to(upright(experts + expert), (tok_count, 128))

        def merge(t, h, i):
            source = order[t]
            back_copy(source, h, i).wait_recv()
            total = None
            for k, block in enumerate((done[source, h, y, :, cols[i]], back_in[source, h, :, cols[i]])):
                scale = jnp.concatenate([shares[t, h, k]] * (step_cols // 128), axis=1)
                term = scale * jnp.dot(spread[t, h, k], block, preferred_element_type=jnp.float32)
                total = term if total is None else total + term
            for way in comes[t]:
                side, arrival = ret_arrival(source, h, i, way)
                arrival.wait_recv()
                total = total + ret_in[side, source, h, :, cols[i]].astype(jnp.float32)
            if t:
                ret_out[source, h, :, cols[i]] = total.astype(jnp.bfloat16)
                ret_copy(source, h, i, leaves[t]).start()
            else:
                last[h, :, cols[i]] = total.astype(jnp.bfloat16)
                pl.when(core != h)(lambda: last_copy(h, i).start())

        def near(t, h, i):
            hop(z, h, i, 0 if at_end else 1).start()

        def far(t, h, i):
            hop(z, h, i, 0).start()

        def own_back(t, h, i):
            back_copy(z, h, i).start()

        stages = (send_rows, share_rows, up, out, add, turn_over, merge, near, far, own_back)
        for number in plan:
            stages[number // 1000](number // 100 % 10, number // 10 % 10, number % 10)
        for t in range(LINE):
            source = order[t]
            for h in range(2):
                for i in range(PARTS):
                    for way in passes[t]:
                        hop(source, h, i, way).wait_send()
                    cross_copy(source, h, i).wait_send()
                    for column in range(2):
                        pair_move(source, h, core, column, i).wait_send()
                    back_copy(source, h, i).wait_send()
                    if t:
                        ret_copy(source, h, i, leaves[t]).wait_send()
                for i in range(BANDS):
                    part_copy(source, h, i).wait_send()

    for k in range(len(peers)):
        meta_copy(k).start()
    mate_copy.wait_recv()
    meta_arrival(z, 1 - core).wait_recv()
    pl.when(outer)(lambda: run(OUTER_PLAN, OUTER_TURNS, True))
    pl.when(jnp.logical_not(outer))(lambda: run(INNER_PLAN, INNER_TURNS, False))
    out_ref[:, mine] = last[core]
    for i in range(PARTS):
        last_copy(1 - core, i).wait_recv()
    out_ref[:, other] = last_in[...]
    mate_copy.wait_send()
    for k in range(len(peers)):
        meta_copy(k).wait_send()
    for i in range(PARTS):
        last_copy(1 - core, i).wait_send()


def fused(tokens, norm_gain, expert_ids, route_weights, gate_proj, linear_proj, down_proj):
    tok_count, width = tokens.shape
    picks = expert_ids.shape[1]
    experts = 2 * LINE
    capacity = 2 * tok_count * picks // experts
    ff = gate_proj.shape[2]
    wide, dma = jnp.bfloat16, pltpu.SemaphoreType.DMA
    inside, outside = pl.BlockSpec(memory_space=pltpu.VMEM), pl.BlockSpec(memory_space=pl.ANY)
    return pl.pallas_call(
        kernel,
        out_shape=jax.ShapeDtypeStruct((tok_count, width), wide),
        in_specs=[inside] * 3 + [outside] * 4,
        out_specs=inside,
        scratch_shapes=[
            pltpu.VMEM((tok_count, width), wide),
            pltpu.VMEM((width, ff), wide),
            pltpu.VMEM((width, ff), wide),
            pltpu.VMEM((ff, width), wide),
            pltpu.VMEM((tok_count, width // 2), wide),
            pltpu.VMEM((LINE, 2, tok_count, width // 2), wide),
            pltpu.VMEM((LINE, 2, 2 * experts, tok_count), jnp.float32),
            pltpu.VMEM((LINE, 2, 2 * capacity, tok_count), wide),
            pltpu.VMEM((LINE, 2, 2, tok_count, capacity), wide),
            pltpu.VMEM((LINE, 2, 2, tok_count, 128), jnp.float32),
            pltpu.VMEM((LINE, 2, 2, 2, capacity, width // 2), wide),
            pltpu.VMEM((LINE, 2, capacity, width // 2), wide),
            pltpu.VMEM((LINE, 2, 2 * capacity, ff), wide),
            pltpu.VMEM((LINE, 2, 2, 2, capacity, width // 2), wide),
            pltpu.VMEM((LINE, 2, 2, capacity, width // 2), wide),
            pltpu.VMEM((LINE, 2, 2, capacity, width // 2), wide),
            pltpu.VMEM((LINE, 2, capacity, width // 2), wide),
            pltpu.VMEM((2, LINE, 2, tok_count, width // 2), wide),
            pltpu.VMEM((LINE, 2, tok_count, width // 2), wide),
            pltpu.VMEM((2, tok_count, width // 2), wide),
            pltpu.VMEM((tok_count, width // 2), wide),
            dma((4,)),
            dma((1,)), dma((1,)),
            dma((LINE, 2, PARTS, 2)), dma((LINE, 2, PARTS)),
            dma((2 * LINE - 1,)), dma((LINE, 2)),
            dma((LINE, 2, PARTS)), dma((LINE, 2, PARTS)),
            dma((LINE, 2, 2, PARTS)), dma((LINE, 2, 2, PARTS)),
            dma((LINE, 2, BANDS)), dma((LINE, 2, BANDS)),
            dma((LINE, 2, PARTS)), dma((LINE, 2, PARTS)),
            dma((LINE, 2, PARTS)), dma((2, LINE, 2, PARTS)),
            dma((PARTS,)), dma((PARTS,)),
        ],
        compiler_params=pltpu.CompilerParams(
            collective_id=0, has_side_effects=True, vmem_limit_bytes=60 * 1024 * 1024
        ),
        name="experts",
    )(
        expert_ids.T, route_weights.T, norm_gain.reshape(1, width), tokens,
        gate_proj[0], linear_proj[0], down_proj[0],
    )


def solution(mesh):
    placed = (
        P(("grp", "ep", "tp"), None),
        P(),
        P(("grp", "ep", "tp"), None),
        P(("grp", "ep", "tp"), None),
        P("ep", None, "tp"),
        P("ep", None, "tp"),
        P("ep", "tp", None),
    )
    along = [device.coords[2] for device in mesh.devices[0, :, 0]]
    planned = along == [index // 2 for index in range(2 * LINE)] and mesh.shape["tp"] == 2
    return jax.shard_map(
        fused if planned else shards,
        mesh=mesh,
        in_specs=placed,
        out_specs=P(("grp", "ep", "tp"), None),
        check_vma=False,
    )
```

```python
import functools

import jax
import jax.numpy as jnp
from jax import lax
from jax.experimental import pallas as pl
from jax.experimental.pallas import tpu as pltpu
from jax.sharding import PartitionSpec as P

MESH = pl.DeviceIdType.MESH
LINE = 4
PARTS = 4
SETTLE = 2
BANDS = 2

OUTER_TURNS = (0, -1, -3, -2)
INNER_TURNS = (0, 1, -2, -1)
OUTER_PLAN = (
    7000, 7001, 7002, 7003, 7010, 7011, 7012, 7013, 10, 11, 12, 13, 5010, 0, 5000, 1,
    2, 3, 1010, 100, 5100, 1011, 1012, 101, 1013, 1000, 102, 1001, 1002, 103, 1003, 1100,
    300, 5300, 1101, 2000, 301, 1102, 1103, 2001, 3000, 302, 1300, 2100, 303, 2101, 1301, 3100,
    310, 3101, 1302, 4100, 5310, 4101, 311, 3001, 4010, 4011, 1303, 4000, 4001, 312, 1310, 2300,
    313, 6100, 6101, 2301, 3300, 200, 3301, 6102, 6103, 1311, 4300, 201, 5200, 4301, 1312, 1313,
    202, 1200, 2310, 203, 6300, 2311, 6301, 3310, 1201, 210, 3311, 6302, 211, 5210, 4310, 6303,
    4311, 1202, 212, 1203, 1210, 213, 2200, 1211, 6310, 2201, 110, 6311, 3200, 6312, 111, 3201,
    6313, 4200, 1212, 4201, 5110, 112, 1213, 1110, 113, 2210, 1111, 6200, 2211, 3210, 6201, 6202,
    3211, 6203, 4210, 4211, 1112, 1113, 2110, 6210, 2111, 6211, 3110, 6212, 3111, 6213, 4110, 4111,
    9000, 9001, 9002, 9003, 9010, 9011, 9012, 9013, 6110, 6111, 6112, 6113, 6000, 6001, 6002, 6003,
    6010, 6011, 6012, 6013,
)
INNER_PLAN = (
    7000, 8000, 7001, 8001, 7002, 8002, 7003, 0, 1, 2, 3, 8003, 8010, 8011, 8012, 8013,
    10, 11, 12, 13, 5000, 5010, 1000, 100, 300, 5300, 5100, 1001, 1002, 101, 301, 1003,
    1010, 102, 302, 1011, 1012, 103, 303, 1013, 1100, 310, 110, 5310, 1300, 5110, 2000, 311,
    111, 1301, 1101, 2001, 1102, 112, 312, 3000, 1302, 1103, 3001, 313, 113, 1303, 4010, 4000,
    4001, 1310, 4011, 2100, 200, 2101, 1311, 2300, 201, 2301, 3300, 1312, 202, 3301, 1313, 1110,
    1111, 1112, 203, 4300, 5200, 4301, 1113, 3100, 2310, 210, 2311, 1200, 1201, 1202, 3310, 211,
    1203, 3311, 212, 4310, 5210, 4311, 2110, 2200, 2201, 213, 7010, 7011, 7012, 7013, 1210, 3200,
    1211, 3201, 1212, 2111, 4200, 4201, 3110, 3111, 6300, 3101, 4100, 4101, 4110, 4111, 9000, 9001,
    9002, 9003, 9010, 9011, 9012, 9013, 6301, 1213, 6302, 2210, 2211, 6303, 3210, 3211, 4210, 6310,
    4211, 6311, 6312, 6313, 6000, 6001, 6200, 6002, 6003, 6201, 6202, 6100, 6203, 6101, 6210, 6102,
    6211, 6103, 6212, 6110, 6213, 6111, 6010, 6112, 6011, 6113, 6012, 6013,
)


def shards(tokens, norm_gain, expert_ids, route_weights, gate_proj, linear_proj, down_proj):
    tok_count, width = tokens.shape
    picks = expert_ids.shape[1]
    experts = lax.axis_size("ep")
    capacity = 2 * tok_count * picks // experts
    values = tokens.astype(jnp.float32)
    normed = (
        values * lax.rsqrt(jnp.mean(values * values, axis=-1, keepdims=True) + 1e-06) * norm_gain
    ).astype(jnp.bfloat16)
    flat = expert_ids.reshape(-1)
    onehot = (flat[:, None] == jnp.arange(experts, dtype=jnp.int32)[None, :]).astype(jnp.int32)
    slots = jnp.sum((jnp.cumsum(onehot, axis=0) - 1) * onehot, axis=1)
    where = flat * capacity + slots
    buffer = (
        jnp.zeros((experts * capacity, width), jnp.bfloat16)
        .at[where]
        .set(jnp.repeat(normed, picks, axis=0))
    )
    arrived = lax.all_to_all(buffer, "ep", split_axis=0, concat_axis=0, tiled=True)
    rows = lax.all_gather(arrived, "tp", axis=0, tiled=True)
    gate_pre = jnp.dot(rows, gate_proj[0], preferred_element_type=jnp.float32)
    lin_pre = jnp.dot(rows, linear_proj[0], preferred_element_type=jnp.float32)
    glu = jnp.minimum(gate_pre, 7.0)
    lin = jnp.clip(lin_pre, -7.0, 7.0)
    hidden = (glu * jax.nn.sigmoid(1.702 * glu) * (lin + 1.0)).astype(jnp.bfloat16)
    rows = hidden
    summed = lax.psum_scatter(
        jnp.dot(rows, down_proj[0], preferred_element_type=jnp.float32).astype(jnp.bfloat16),
        "tp",
        scatter_dimension=0,
        tiled=True,
    )
    returned = lax.all_to_all(summed, "ep", split_axis=0, concat_axis=0, tiled=True)
    picked = returned[where].reshape(tok_count, picks, width).astype(jnp.float32)
    return jnp.sum(picked * route_weights[:, :, None], axis=1).astype(jnp.bfloat16)


def kernel(
    ids_hbm, weights_hbm, gain_hbm, tokens_hbm, gate_hbm, linear_hbm, down_hbm, out_ref,
    ids_ref, weights_ref, gain_ref, tokens_ref, gate, linear, down, mate, tok, meta, pick, spread, shares, rows, cross, hidden, part, part_in, done,
    back_in, ret_in, ret_out, last, last_in,
    load_sem, mate_send, mate_recv, tok_send, tok_recv, meta_send, meta_recv, cross_send, cross_recv,
    pair_send, pair_recv, part_send, part_recv, back_send, back_recv, ret_send, ret_recv,
    last_send, last_recv,
):
    ep, core = lax.axis_index("ep"), lax.axis_index("tp")
    z, y = ep // 2, ep % 2
    experts = 2 * LINE
    tok_count, width = tokens_hbm.shape
    half = width // 2
    capacity = cross.shape[2]
    ff = gate.shape[1]
    step_cols, step_band, unit = half // PARTS, half // BANDS, 256
    cols = [pl.ds(i * step_cols, step_cols) for i in range(PARTS)]
    whole = pl.ds(0, half)
    here, there = z * 2 + y, z * 2 + 1 - y
    mine = pl.ds(pl.multiple_of(core * half, half), half)
    other = pl.ds(pl.multiple_of((1 - core) * half, half), half)
    at_y = {"ep": there}
    at_core = {"tp": 1 - core}
    outwards = jnp.where(z < LINE // 2, -1, 1)
    outer = (z == 0) | (z == LINE - 1)

    def at_z(other):
        return {"ep": other * 2 + y}

    def remote(source, target, send, recv, device):
        return pltpu.make_async_remote_copy(
            src_ref=source, dst_ref=target, send_sem=send, recv_sem=recv,
            device_id=device, device_id_type=MESH,
        )

    peers = [at_core] + [
        {"ep": lax.rem(z + step, LINE) * 2 + y, "tp": tp} for step in range(1, LINE) for tp in range(2)
    ]
    loads = [
        pltpu.make_async_copy(source, target, load_sem.at[i])
        for i, (source, target) in enumerate(((gate_hbm, gate), (linear_hbm, linear), (down_hbm, down)))
    ]
    fetches = [
        pltpu.make_async_copy(source, target, load_sem.at[3 + i])
        for i, (source, target) in enumerate(
            ((tokens_hbm, tokens_ref), (gain_hbm, gain_ref), (ids_hbm, ids_ref), (weights_hbm, weights_ref))
        )
    ]
    for fetch in fetches:
        fetch.start()
    barrier = pltpu.get_barrier_semaphore()
    for device in peers + [at_y]:
        pl.semaphore_signal(barrier, 1, device_id=device, device_id_type=MESH)

    def normalize(i, _):
        span = pl.ds(pl.multiple_of(i * 32, 32), 32)
        values = tokens_ref[span, :].astype(jnp.float32)
        scale = lax.rsqrt(jnp.mean(values * values, axis=-1, keepdims=True) + 1e-06)
        mate[span, :] = (tokens_ref[span, other].astype(jnp.float32) * scale * gain_ref[:, other]).astype(
            jnp.bfloat16
        )
        tok[z, core, span, :] = (tokens_ref[span, mine].astype(jnp.float32) * scale * gain_ref[:, mine]).astype(
            jnp.bfloat16
        )
        return 0

    for fetch in fetches:
        fetch.wait()
    for load in loads:
        load.start()
    lax.fori_loop(0, tok_count // 32, normalize, 0)
    pl.semaphore_wait(barrier, len(peers) + 1)
    mate_copy = remote(mate, tok.at[z, core], mate_send.at[0], mate_recv.at[0], at_core)
    mate_copy.start()
    names = lax.broadcasted_iota(jnp.int32, (experts, tok_count), 0)
    share = jnp.zeros((experts, tok_count), jnp.float32)
    chosen = jnp.zeros((experts, tok_count), jnp.float32)
    for choice in range(ids_ref.shape[0]):
        same = ids_ref[choice : choice + 1, :] == names
        share = share + jnp.where(same, weights_ref[choice : choice + 1, :], 0.0)
        chosen = chosen + jnp.where(same, 1.0, 0.0)
    first = lax.broadcasted_iota(jnp.int32, (tok_count, tok_count), 0)
    second = lax.broadcasted_iota(jnp.int32, (tok_count, tok_count), 1)
    before = jnp.where(first < second, 1.0, 0.0).astype(jnp.bfloat16)
    slots = jnp.dot(chosen.astype(jnp.bfloat16), before, preferred_element_type=jnp.float32)
    meta[z, core, 0:experts, :] = jnp.where(chosen > 0.5, slots, -1.0)
    meta[z, core, experts : 2 * experts, :] = share

    def meta_copy(k):
        block = meta.at[z, core]
        return remote(block, block, meta_send.at[k], meta_recv.at[z, core], peers[k])

    def meta_arrival(source, h):
        block = meta.at[source, h]
        return remote(block, block, meta_send.at[0], meta_recv.at[source, h], at_core)

    def piece(i):
        return whole if i is None else cols[i]

    def first(i):
        return 0 if i is None else i

    def hop(source, h, i, way):
        block = tok.at[source, h, :, piece(i)]
        target = z + outwards if way else z - outwards
        return remote(
            block, block, tok_send.at[source, h, way], tok_recv.at[source, h, first(i)], at_z(target)
        )

    def cross_copy(source, h, i):
        return remote(
            cross.at[source, h, :, piece(i)], rows.at[source, h, core, y, :, piece(i)],
            cross_send.at[source, h], cross_recv.at[source, h, first(i)], at_y,
        )

    def cross_arrival(source, h, i):
        return remote(
            cross.at[source, h, :, cols[i]], rows.at[source, h, core, 1 - y, :, cols[i]],
            cross_send.at[source, h], cross_recv.at[source, h, i], at_y,
        )

    def pair_move(source, h, owner, span):
        block = rows.at[source, h, owner, :, :, span]
        return remote(block, block, pair_send.at[source, h], pair_recv.at[source, h], at_core)

    def part_copy(source, h, i):
        if i is None:
            band = whole
        elif isinstance(i, int):
            band = pl.ds(i * step_band, step_band)
        else:
            band = pl.ds(pl.multiple_of(i * step_band, step_band), step_band)
        return remote(
            part.at[source, h, 1 - core, :, :, band], part_in.at[source, h, :, :, band],
            part_send.at[source, h], part_recv.at[source, h, first(i)], at_core,
        )

    def back_copy(source, h, i):
        return remote(
            done.at[source, h, 1 - y, :, piece(i)], back_in.at[source, h, :, piece(i)],
            back_send.at[source, h], back_recv.at[source, h, first(i)], at_y,
        )

    def ret_copy(source, h, i, way):
        step = outwards if way else -outwards
        side = jnp.where(step > 0, 0, 1)
        return remote(
            ret_out.at[source, h, :, piece(i)], ret_in.at[side, source, h, :, piece(i)],
            ret_send.at[source, h], ret_recv.at[side, source, h, first(i)], at_z(z + step),
        )

    def ret_arrival(source, h, i, way):
        step = -outwards if way else outwards
        side = jnp.where(step > 0, 0, 1)
        return side, remote(
            ret_out.at[source, h, :, cols[i]], ret_in.at[side, source, h, :, cols[i]],
            ret_send.at[source, h], ret_recv.at[side, source, h, i], at_z(z - step),
        )

    def last_copy(h, i):
        return remote(
            last.at[h, :, cols[i]], last_in.at[:, cols[i]], last_send.at[i], last_recv.at[i], at_core
        )

    def run(plan, turns, at_end):
        order = [z + outwards * turn for turn in turns]
        if at_end:
            passes = [(0,), (), (), ()]
            comes = [(0,), (), (), ()]
        else:
            passes = [(1, 0)] + [(0,) if turn > 0 else (1,) for turn in turns[1:]]
            comes = [(0, 1)] + [(0,) if turn > 0 else (1,) for turn in turns[1:]]
        leaves = [None] + [1 if turn > 0 else 0 for turn in turns[1:]]
        waited = [False, False]

        def send_rows(t, h, i):
            source = order[t]
            if t:
                hop(source, h, i, 0).wait_recv()
                for way in passes[t]:
                    hop(source, h, i, way).start()
            if i == 0:
                if t:
                    meta_arrival(source, h).wait_recv()
                place = lax.broadcasted_iota(jnp.int32, (capacity, tok_count), 0).astype(jnp.float32)
                for k, expert in enumerate((there, here)):
                    pick[t, h, k * capacity : (k + 1) * capacity, :] = (
                        meta[source, h, pl.ds(expert, 1), :] == place
                    ).astype(jnp.bfloat16)
            both = jnp.dot(
                pick[t, h], tok[source, h, :, cols[i]], preferred_element_type=jnp.float32
            ).astype(jnp.bfloat16)
            cross[source, h, :, cols[i]] = both[:capacity]
            cross_copy(source, h, i).start()
            rows[source, h, core, y, :, cols[i]] = both[capacity:]

        def share_rows(t, h, i):
            source = order[t]
            cross_arrival(source, h, i).wait_recv()
            pair_move(source, h, core, cols[i]).start()

        def up(t, h, i):
            source = order[t]
            blocks = range(h, h + 1) if t else range(2)
            for block in blocks if i == 0 else ():
                pair_move(source, block, 1 - core, whole).wait_recv()
            if not waited[0]:
                waited[0] = True
                loads[0].wait()
                loads[1].wait()
            span_h = slice(blocks[0], blocks[-1] + 1)

            def units(j, _):
                span = pl.ds(j * unit if isinstance(j, int) else pl.multiple_of(j * unit, unit), unit)
                low = rows[source, span_h, 0].reshape(len(blocks) * 2 * capacity, half)
                high = rows[source, span_h, 1].reshape(len(blocks) * 2 * capacity, half)

                def through(matrix):
                    return jnp.dot(low, matrix[:half, span], preferred_element_type=jnp.float32) + jnp.dot(
                        high, matrix[half:, span], preferred_element_type=jnp.float32
                    )

                glu = jnp.minimum(through(gate), 7.0)
                lin = jnp.clip(through(linear), -7.0, 7.0)
                hidden[t, span_h, :, span] = (
                    (glu * jax.nn.sigmoid(1.702 * glu) * (lin + 1.0))
                    .astype(jnp.bfloat16)
                    .reshape(len(blocks), 2 * capacity, unit)
                )
                return 0

            if i == 0:
                lax.fori_loop(0, ff // unit - 1, units, 0)
            else:
                units(ff // unit - 1, 0)

        def out(t, h, i):
            source = order[t]
            blocks = range(h, h + 1) if t else range(2)
            span_h = slice(blocks[0], blocks[-1] + 1)
            if not waited[1]:
                waited[1] = True
                loads[2].wait()

            def bands(side, send):
                def go(j, _):
                    start = side * half + j * step_band
                    span = pl.ds(pl.multiple_of(start, step_band), step_band)
                    inputs = hidden[t, span_h].reshape(len(blocks) * 2 * capacity, ff)
                    part[source, span_h, side, :, :, pl.ds(pl.multiple_of(j * step_band, step_band), step_band)] = (
                        jnp.dot(inputs, down[:, span], preferred_element_type=jnp.float32)
                        .astype(jnp.bfloat16)
                        .reshape(len(blocks), 2, capacity, step_band)
                    )
                    if send:
                        for block in blocks:
                            part_copy(source, block, j).start()
                    return 0

                lax.fori_loop(0, BANDS, go, 0)

            bands(core if i else 1 - core, i == 0)

        def add(t, h, i):
            source = order[t]
            part_copy(source, h, i).wait_recv()
            band = pl.ds(i * step_band, step_band)
            done[source, h, :, :, band] = (
                part[source, h, core, :, :, band].astype(jnp.float32)
                + part_in[source, h, :, :, band].astype(jnp.float32)
            ).astype(jnp.bfloat16)
            if t:
                for j in range(i * PARTS // BANDS, (i + 1) * PARTS // BANDS):
                    back_copy(source, h, j).start()

        def turn_over(t, h, i):
            source = order[t]
            eye = lax.broadcasted_iota(jnp.int32, (tok_count, tok_count), 0) == lax.broadcasted_iota(
                jnp.int32, (tok_count, tok_count), 1
            )
            lane = lax.broadcasted_iota(jnp.int32, (tok_count, capacity), 1).astype(jnp.float32)

            def upright(row):
                return jnp.sum(jnp.where(eye, meta[source, h, pl.ds(row, 1), :], 0.0), axis=1, keepdims=True)

            for k, expert in enumerate((here, there)):
                spread[t, h, k] = (upright(expert) == lane).astype(jnp.bfloat16)
                shares[t, h, k] = jnp.broadcast_to(upright(experts + expert), (tok_count, 128))

        def merge(t, h, i):
            source = order[t]
            back_copy(source, h, i).wait_recv()
            total = None
            for k, block in enumerate((done[source, h, y, :, cols[i]], back_in[source, h, :, cols[i]])):
                scale = jnp.concatenate([shares[t, h, k]] * (step_cols // 128), axis=1)
                term = scale * jnp.dot(spread[t, h, k], block, preferred_element_type=jnp.float32)
                total = term if total is None else total + term
            for way in comes[t]:
                side, arrival = ret_arrival(source, h, i, way)
                arrival.wait_recv()
                total = total + ret_in[side, source, h, :, cols[i]].astype(jnp.float32)
            if t:
                ret_out[source, h, :, cols[i]] = total.astype(jnp.bfloat16)
                ret_copy(source, h, i, leaves[t]).start()
            else:
                last[h, :, cols[i]] = total.astype(jnp.bfloat16)
                pl.when(core != h)(lambda: last_copy(h, i).start())

        def near(t, h, i):
            hop(z, h, i, 0 if at_end else 1).start()

        def far(t, h, i):
            hop(z, h, i, 0).start()

        def own_back(t, h, i):
            back_copy(z, h, i).start()

        def settle():
            for t in range(LINE):
                source = order[t]
                for h in range(2):
                    for way in passes[t]:
                        hop(source, h, None, way).wait_send()
                    cross_copy(source, h, None).wait_send()
                    pair_move(source, h, core, whole).wait_send()
                    part_copy(source, h, None).wait_send()
                    back_copy(source, h, None).wait_send()

        stages = (send_rows, share_rows, up, out, add, turn_over, merge, near, far, own_back)
        for place, number in enumerate(plan):
            if place == len(plan) - SETTLE:
                settle()
            stages[number // 1000](number // 100 % 10, number // 10 % 10, number % 10)
        for t in range(1, LINE):
            for h in range(2):
                ret_copy(order[t], h, None, leaves[t]).wait_send()

    for k in range(len(peers)):
        meta_copy(k).start()
    mate_copy.wait_recv()
    meta_arrival(z, 1 - core).wait_recv()
    pl.when(outer)(lambda: run(OUTER_PLAN, OUTER_TURNS, True))
    pl.when(jnp.logical_not(outer))(lambda: run(INNER_PLAN, INNER_TURNS, False))
    out_ref[:, mine] = last[core]
    for i in range(PARTS):
        last_copy(1 - core, i).wait_recv()
    out_ref[:, other] = last_in[...]
    mate_copy.wait_send()
    for k in range(len(peers)):
        meta_copy(k).wait_send()
    for i in range(PARTS):
        last_copy(1 - core, i).wait_send()


def fused(tokens, norm_gain, expert_ids, route_weights, gate_proj, linear_proj, down_proj):
    tok_count, width = tokens.shape
    picks = expert_ids.shape[1]
    experts = 2 * LINE
    capacity = 2 * tok_count * picks // experts
    ff = gate_proj.shape[2]
    wide, dma = jnp.bfloat16, pltpu.SemaphoreType.DMA
    inside, outside = pl.BlockSpec(memory_space=pltpu.VMEM), pl.BlockSpec(memory_space=pl.ANY)
    return pl.pallas_call(
        kernel,
        out_shape=jax.ShapeDtypeStruct((tok_count, width), wide),
        in_specs=[outside] * 7,
        out_specs=inside,
        scratch_shapes=[
            pltpu.VMEM((picks, tok_count), jnp.int32),
            pltpu.VMEM((picks, tok_count), jnp.float32),
            pltpu.VMEM((1, width), jnp.float32),
            pltpu.VMEM((tok_count, width), wide),
            pltpu.VMEM((width, ff), wide),
            pltpu.VMEM((width, ff), wide),
            pltpu.VMEM((ff, width), wide),
            pltpu.VMEM((tok_count, width // 2), wide),
            pltpu.VMEM((LINE, 2, tok_count, width // 2), wide),
            pltpu.VMEM((LINE, 2, 2 * experts, tok_count), jnp.float32),
            pltpu.VMEM((LINE, 2, 2 * capacity, tok_count), wide),
            pltpu.VMEM((LINE, 2, 2, tok_count, capacity), wide),
            pltpu.VMEM((LINE, 2, 2, tok_count, 128), jnp.float32),
            pltpu.VMEM((LINE, 2, 2, 2, capacity, width // 2), wide),
            pltpu.VMEM((LINE, 2, capacity, width // 2), wide),
            pltpu.VMEM((LINE, 2, 2 * capacity, ff), wide),
            pltpu.VMEM((LINE, 2, 2, 2, capacity, width // 2), wide),
            pltpu.VMEM((LINE, 2, 2, capacity, width // 2), wide),
            pltpu.VMEM((LINE, 2, 2, capacity, width // 2), wide),
            pltpu.VMEM((LINE, 2, capacity, width // 2), wide),
            pltpu.VMEM((2, LINE, 2, tok_count, width // 2), wide),
            pltpu.VMEM((LINE, 2, tok_count, width // 2), wide),
            pltpu.VMEM((2, tok_count, width // 2), wide),
            pltpu.VMEM((tok_count, width // 2), wide),
            dma((7,)),
            dma((1,)), dma((1,)),
            dma((LINE, 2, 2)), dma((LINE, 2, PARTS)),
            dma((2 * LINE - 1,)), dma((LINE, 2)),
            dma((LINE, 2)), dma((LINE, 2, PARTS)),
            dma((LINE, 2)), dma((LINE, 2)),
            dma((LINE, 2)), dma((LINE, 2, BANDS)),
            dma((LINE, 2)), dma((LINE, 2, PARTS)),
            dma((LINE, 2)), dma((2, LINE, 2, PARTS)),
            dma((PARTS,)), dma((PARTS,)),
        ],
        compiler_params=pltpu.CompilerParams(
            collective_id=0, has_side_effects=True, vmem_limit_bytes=60 * 1024 * 1024
        ),
        name="experts",
    )(
        expert_ids.T, route_weights.T, norm_gain.reshape(1, width), tokens,
        gate_proj[0], linear_proj[0], down_proj[0],
    )


def solution(mesh):
    placed = (
        P(("grp", "ep", "tp"), None),
        P(),
        P(("grp", "ep", "tp"), None),
        P(("grp", "ep", "tp"), None),
        P("ep", None, "tp"),
        P("ep", None, "tp"),
        P("ep", "tp", None),
    )
    along = [device.coords[2] for device in mesh.devices[0, :, 0]]
    planned = along == [index // 2 for index in range(2 * LINE)] and mesh.shape["tp"] == 2
    return jax.shard_map(
        fused if planned else shards,
        mesh=mesh,
        in_specs=placed,
        out_specs=P(("grp", "ep", "tp"), None),
        check_vma=False,
    )
```

```python
import functools

import jax
import jax.numpy as jnp
from jax import lax
from jax.experimental import pallas as pl
from jax.experimental.pallas import tpu as pltpu
from jax.sharding import PartitionSpec as P

MESH = pl.DeviceIdType.MESH
LINE = 4
PARTS = 4
SETTLE = 2
BANDS = 2

OUTER_TURNS = (0, -1, -3, -2)
INNER_TURNS = (0, 1, -2, -1)
OUTER_PLAN = (
    7000, 7001, 7002, 7003, 7010, 7011, 7012, 7013, 10, 11, 12, 13, 5010, 0, 5000, 1,
    2, 3, 1010, 100, 5100, 1011, 1012, 101, 1013, 1000, 102, 1001, 1002, 103, 1003, 1100,
    300, 5300, 1101, 2000, 301, 1102, 1103, 2001, 3000, 302, 1300, 2100, 303, 2101, 1301, 3100,
    310, 3101, 1302, 4100, 5310, 4101, 311, 3001, 4010, 4011, 1303, 4000, 4001, 312, 1310, 2300,
    313, 6100, 6101, 2301, 3300, 200, 3301, 6102, 6103, 1311, 4300, 201, 5200, 4301, 1312, 1313,
    202, 1200, 2310, 203, 6300, 2311, 6301, 3310, 1201, 210, 3311, 6302, 211, 5210, 4310, 6303,
    4311, 1202, 212, 1203, 1210, 213, 2200, 1211, 6310, 2201, 110, 6311, 3200, 6312, 111, 3201,
    6313, 4200, 1212, 4201, 5110, 112, 1213, 1110, 113, 2210, 1111, 6200, 2211, 3210, 6201, 6202,
    3211, 6203, 4210, 4211, 1112, 1113, 2110, 6210, 2111, 6211, 3110, 6212, 3111, 6213, 4110, 4111,
    9000, 9001, 9002, 9003, 9010, 9011, 9012, 9013, 6110, 6111, 6112, 6113, 6000, 6001, 6002, 6003,
    6010, 6011, 6012, 6013,
)
INNER_PLAN = (
    7000, 8000, 7001, 8001, 7002, 8002, 7003, 0, 1, 2, 3, 8003, 8010, 8011, 8012, 8013,
    10, 11, 12, 13, 5000, 5010, 1000, 100, 300, 5300, 5100, 1001, 1002, 101, 301, 1003,
    1010, 102, 302, 1011, 1012, 103, 303, 1013, 1100, 310, 110, 5310, 1300, 5110, 2000, 311,
    111, 1301, 1101, 2001, 1102, 112, 312, 3000, 1302, 1103, 3001, 313, 113, 1303, 4010, 4000,
    4001, 1310, 4011, 2100, 200, 2101, 1311, 2300, 201, 2301, 3300, 1312, 202, 3301, 1313, 1110,
    1111, 1112, 203, 4300, 5200, 4301, 1113, 3100, 2310, 210, 2311, 1200, 1201, 1202, 3310, 211,
    1203, 3311, 212, 4310, 5210, 4311, 2110, 2200, 2201, 213, 7010, 7011, 7012, 7013, 1210, 3200,
    1211, 3201, 1212, 2111, 4200, 4201, 3110, 3111, 6300, 3101, 4100, 4101, 4110, 4111, 9000, 9001,
    9002, 9003, 9010, 9011, 9012, 9013, 6301, 1213, 6302, 2210, 2211, 6303, 3210, 3211, 4210, 6310,
    4211, 6311, 6312, 6313, 6000, 6001, 6200, 6002, 6003, 6201, 6202, 6100, 6203, 6101, 6210, 6102,
    6211, 6103, 6212, 6110, 6213, 6111, 6010, 6112, 6011, 6113, 6012, 6013,
)


def shards(tokens, norm_gain, expert_ids, route_weights, gate_proj, linear_proj, down_proj):
    tok_count, width = tokens.shape
    picks = expert_ids.shape[1]
    experts = lax.axis_size("ep")
    capacity = 2 * tok_count * picks // experts
    values = tokens.astype(jnp.float32)
    normed = (
        values * lax.rsqrt(jnp.mean(values * values, axis=-1, keepdims=True) + 1e-06) * norm_gain
    ).astype(jnp.bfloat16)
    flat = expert_ids.reshape(-1)
    onehot = (flat[:, None] == jnp.arange(experts, dtype=jnp.int32)[None, :]).astype(jnp.int32)
    slots = jnp.sum((jnp.cumsum(onehot, axis=0) - 1) * onehot, axis=1)
    where = flat * capacity + slots
    buffer = (
        jnp.zeros((experts * capacity, width), jnp.bfloat16)
        .at[where]
        .set(jnp.repeat(normed, picks, axis=0))
    )
    arrived = lax.all_to_all(buffer, "ep", split_axis=0, concat_axis=0, tiled=True)
    rows = lax.all_gather(arrived, "tp", axis=0, tiled=True)
    gate_pre = jnp.dot(rows, gate_proj[0], preferred_element_type=jnp.float32)
    lin_pre = jnp.dot(rows, linear_proj[0], preferred_element_type=jnp.float32)
    glu = jnp.minimum(gate_pre, 7.0)
    lin = jnp.clip(lin_pre, -7.0, 7.0)
    hidden = (glu * jax.nn.sigmoid(1.702 * glu) * (lin + 1.0)).astype(jnp.bfloat16)
    rows = hidden
    summed = lax.psum_scatter(
        jnp.dot(rows, down_proj[0], preferred_element_type=jnp.float32).astype(jnp.bfloat16),
        "tp",
        scatter_dimension=0,
        tiled=True,
    )
    returned = lax.all_to_all(summed, "ep", split_axis=0, concat_axis=0, tiled=True)
    picked = returned[where].reshape(tok_count, picks, width).astype(jnp.float32)
    return jnp.sum(picked * route_weights[:, :, None], axis=1).astype(jnp.bfloat16)


def kernel(
    ids_hbm, weights_hbm, gain_hbm, tokens_hbm, gate_hbm, linear_hbm, down_hbm, out_ref,
    ids_ref, weights_ref, gain_ref, tokens_ref, gate, linear, down, mate, tok, meta, pick, spread, shares, rows, cross, hidden, part, part_in, done,
    back_in, ret_in, ret_out, last, last_in,
    load_sem, mate_send, mate_recv, tok_send, tok_recv, meta_send, meta_recv, cross_send, cross_recv,
    pair_send, pair_recv, part_send, part_recv, back_send, back_recv, ret_send, ret_recv,
    last_send, last_recv,
):
    ep, core = lax.axis_index("ep"), lax.axis_index("tp")
    z, y = ep // 2, ep % 2
    experts = 2 * LINE
    tok_count, width = tokens_hbm.shape
    half = width // 2
    capacity = cross.shape[2]
    ff = gate.shape[1]
    step_cols, step_band, unit = half // PARTS, half // BANDS, 256
    cols = [pl.ds(i * step_cols, step_cols) for i in range(PARTS)]
    whole = pl.ds(0, half)
    here, there = z * 2 + y, z * 2 + 1 - y
    mine = pl.ds(pl.multiple_of(core * half, half), half)
    other = pl.ds(pl.multiple_of((1 - core) * half, half), half)
    at_y = {"ep": there}
    at_core = {"tp": 1 - core}
    outwards = jnp.where(z < LINE // 2, -1, 1)
    outer = (z == 0) | (z == LINE - 1)

    def at_z(other):
        return {"ep": other * 2 + y}

    def remote(source, target, send, recv, device):
        return pltpu.make_async_remote_copy(
            src_ref=source, dst_ref=target, send_sem=send, recv_sem=recv,
            device_id=device, device_id_type=MESH,
        )

    peers = [at_core] + [
        {"ep": lax.rem(z + step, LINE) * 2 + y, "tp": tp} for step in range(1, LINE) for tp in range(2)
    ]
    loads = [
        pltpu.make_async_copy(source, target, load_sem.at[i])
        for i, (source, target) in enumerate(((gate_hbm, gate), (linear_hbm, linear), (down_hbm, down)))
    ]
    fetches = [
        pltpu.make_async_copy(source, target, load_sem.at[3 + i])
        for i, (source, target) in enumerate(
            ((tokens_hbm, tokens_ref), (gain_hbm, gain_ref), (ids_hbm, ids_ref), (weights_hbm, weights_ref))
        )
    ]
    for fetch in fetches:
        fetch.start()
    barrier = pltpu.get_barrier_semaphore()
    for device in peers + [at_y]:
        pl.semaphore_signal(barrier, 1, device_id=device, device_id_type=MESH)

    def normalize(i, _):
        span = pl.ds(pl.multiple_of(i * 32, 32), 32)
        values = tokens_ref[span, :].astype(jnp.float32)
        scale = lax.rsqrt(jnp.mean(values * values, axis=-1, keepdims=True) + 1e-06)
        mate[span, :] = (tokens_ref[span, other].astype(jnp.float32) * scale * gain_ref[:, other]).astype(
            jnp.bfloat16
        )
        tok[z, core, span, :] = (tokens_ref[span, mine].astype(jnp.float32) * scale * gain_ref[:, mine]).astype(
            jnp.bfloat16
        )
        return 0

    for fetch in fetches:
        fetch.wait()
    for load in loads:
        load.start()
    lax.fori_loop(0, tok_count // 32, normalize, 0)
    pl.semaphore_wait(barrier, len(peers) + 1)
    mate_copy = remote(mate, tok.at[z, core], mate_send.at[0], mate_recv.at[0], at_core)
    mate_copy.start()
    names = lax.broadcasted_iota(jnp.int32, (experts, tok_count), 0)
    share = jnp.zeros((experts, tok_count), jnp.float32)
    chosen = jnp.zeros((experts, tok_count), jnp.float32)
    for choice in range(ids_ref.shape[0]):
        same = ids_ref[choice : choice + 1, :] == names
        share = share + jnp.where(same, weights_ref[choice : choice + 1, :], 0.0)
        chosen = chosen + jnp.where(same, 1.0, 0.0)
    first = lax.broadcasted_iota(jnp.int32, (tok_count, tok_count), 0)
    second = lax.broadcasted_iota(jnp.int32, (tok_count, tok_count), 1)
    before = jnp.where(first < second, 1.0, 0.0).astype(jnp.bfloat16)
    slots = jnp.dot(chosen.astype(jnp.bfloat16), before, preferred_element_type=jnp.float32)
    meta[z, core, 0:experts, :] = jnp.where(chosen > 0.5, slots, -1.0)
    meta[z, core, experts : 2 * experts, :] = share

    def meta_copy(k):
        block = meta.at[z, core]
        return remote(block, block, meta_send.at[k], meta_recv.at[z, core], peers[k])

    def meta_arrival(source, h):
        block = meta.at[source, h]
        return remote(block, block, meta_send.at[0], meta_recv.at[source, h], at_core)

    def piece(i):
        return whole if i is None else cols[i]

    def first(i):
        return 0 if i is None else i

    def hop(source, h, i, way):
        block = tok.at[source, h, :, piece(i)]
        target = z + outwards if way else z - outwards
        return remote(
            block, block, tok_send.at[source, h, way], tok_recv.at[source, h, first(i)], at_z(target)
        )

    def cross_copy(source, h, i):
        return remote(
            cross.at[source, h, :, piece(i)], rows.at[source, h, core, y, :, piece(i)],
            cross_send.at[source, h], cross_recv.at[source, h, first(i)], at_y,
        )

    def cross_arrival(source, h, i):
        return remote(
            cross.at[source, h, :, cols[i]], rows.at[source, h, core, 1 - y, :, cols[i]],
            cross_send.at[source, h], cross_recv.at[source, h, i], at_y,
        )

    def pair_move(source, h, owner, span):
        block = rows.at[source, h, owner, :, :, span]
        return remote(block, block, pair_send.at[source, h], pair_recv.at[source, h], at_core)

    def part_copy(source, h, i):
        if i is None:
            band = whole
        elif isinstance(i, int):
            band = pl.ds(i * step_band, step_band)
        else:
            band = pl.ds(pl.multiple_of(i * step_band, step_band), step_band)
        return remote(
            part.at[source, h, 1 - core, :, :, band], part_in.at[source, h, :, :, band],
            part_send.at[source, h], part_recv.at[source, h, first(i)], at_core,
        )

    def back_copy(source, h, i):
        return remote(
            done.at[source, h, 1 - y, :, piece(i)], back_in.at[source, h, :, piece(i)],
            back_send.at[source, h], back_recv.at[source, h, first(i)], at_y,
        )

    def ret_copy(source, h, i, way):
        step = outwards if way else -outwards
        side = jnp.where(step > 0, 0, 1)
        return remote(
            ret_out.at[source, h, :, piece(i)], ret_in.at[side, source, h, :, piece(i)],
            ret_send.at[source, h], ret_recv.at[side, source, h, first(i)], at_z(z + step),
        )

    def ret_arrival(source, h, i, way):
        step = -outwards if way else outwards
        side = jnp.where(step > 0, 0, 1)
        return side, remote(
            ret_out.at[source, h, :, cols[i]], ret_in.at[side, source, h, :, cols[i]],
            ret_send.at[source, h], ret_recv.at[side, source, h, i], at_z(z - step),
        )

    def last_copy(h, i):
        return remote(
            last.at[h, :, cols[i]], last_in.at[:, cols[i]], last_send.at[i], last_recv.at[i], at_core
        )

    def run(plan, turns, at_end):
        order = [z + outwards * turn for turn in turns]
        if at_end:
            passes = [(0,), (), (), ()]
            comes = [(0,), (), (), ()]
        else:
            passes = [(1, 0)] + [(0,) if turn > 0 else (1,) for turn in turns[1:]]
            comes = [(0, 1)] + [(0,) if turn > 0 else (1,) for turn in turns[1:]]
        leaves = [None] + [1 if turn > 0 else 0 for turn in turns[1:]]
        waited = [False, False]

        def send_rows(t, h, i):
            source = order[t]
            if t:
                hop(source, h, i, 0).wait_recv()
                for way in passes[t]:
                    hop(source, h, i, way).start()
            if i == 0:
                if t:
                    meta_arrival(source, h).wait_recv()
                place = lax.broadcasted_iota(jnp.int32, (capacity, tok_count), 0).astype(jnp.float32)
                for k, expert in enumerate((there, here)):
                    pick[t, h, k * capacity : (k + 1) * capacity, :] = (
                        meta[source, h, pl.ds(expert, 1), :] == place
                    ).astype(jnp.bfloat16)
            both = jnp.dot(
                pick[t, h], tok[source, h, :, cols[i]], preferred_element_type=jnp.float32
            ).astype(jnp.bfloat16)
            cross[source, h, :, cols[i]] = both[:capacity]
            cross_copy(source, h, i).start()
            rows[source, h, core, y, :, cols[i]] = both[capacity:]

        def share_rows(t, h, i):
            source = order[t]
            cross_arrival(source, h, i).wait_recv()
            pair_move(source, h, core, cols[i]).start()

        def up(t, h, i):
            source = order[t]
            blocks = range(h, h + 1) if t else range(2)
            for block in blocks if i == 0 else ():
                pair_move(source, block, 1 - core, whole).wait_recv()
            if not waited[0]:
                waited[0] = True
                loads[0].wait()
                loads[1].wait()
            span_h = slice(blocks[0], blocks[-1] + 1)

            def units(j, _):
                span = pl.ds(j * unit if isinstance(j, int) else pl.multiple_of(j * unit, unit), unit)
                low = rows[source, span_h, 0].reshape(len(blocks) * 2 * capacity, half)
                high = rows[source, span_h, 1].reshape(len(blocks) * 2 * capacity, half)

                def through(matrix):
                    return jnp.dot(low, matrix[:half, span], preferred_element_type=jnp.float32) + jnp.dot(
                        high, matrix[half:, span], preferred_element_type=jnp.float32
                    )

                glu = jnp.minimum(through(gate), 7.0)
                lin = jnp.clip(through(linear), -7.0, 7.0)
                hidden[t, span_h, :, span] = (
                    (glu * jax.nn.sigmoid(1.702 * glu) * (lin + 1.0))
                    .astype(jnp.bfloat16)
                    .reshape(len(blocks), 2 * capacity, unit)
                )
                return 0

            if i == 0:
                lax.fori_loop(0, ff // unit - 1, units, 0)
            else:
                units(ff // unit - 1, 0)

        def out(t, h, i):
            source = order[t]
            blocks = range(h, h + 1) if t else range(2)
            span_h = slice(blocks[0], blocks[-1] + 1)
            if not waited[1]:
                waited[1] = True
                loads[2].wait()

            def bands(side, send):
                def go(j, _):
                    start = side * half + j * step_band
                    span = pl.ds(pl.multiple_of(start, step_band), step_band)
                    inputs = hidden[t, span_h].reshape(len(blocks) * 2 * capacity, ff)
                    part[source, span_h, side, :, :, pl.ds(pl.multiple_of(j * step_band, step_band), step_band)] = (
                        jnp.dot(inputs, down[:, span], preferred_element_type=jnp.float32)
                        .astype(jnp.bfloat16)
                        .reshape(len(blocks), 2, capacity, step_band)
                    )
                    if send:
                        for block in blocks:
                            part_copy(source, block, j).start()
                    return 0

                lax.fori_loop(0, BANDS, go, 0)

            bands(core if i else 1 - core, i == 0)

        def add(t, h, i):
            source = order[t]
            part_copy(source, h, i).wait_recv()
            for j in range(i * PARTS // BANDS, (i + 1) * PARTS // BANDS):
                done[source, h, :, :, cols[j]] = (
                    part[source, h, core, :, :, cols[j]].astype(jnp.float32)
                    + part_in[source, h, :, :, cols[j]].astype(jnp.float32)
                ).astype(jnp.bfloat16)
                if t:
                    back_copy(source, h, j).start()

        def turn_over(t, h, i):
            source = order[t]
            eye = lax.broadcasted_iota(jnp.int32, (tok_count, tok_count), 0) == lax.broadcasted_iota(
                jnp.int32, (tok_count, tok_count), 1
            )
            lane = lax.broadcasted_iota(jnp.int32, (tok_count, capacity), 1).astype(jnp.float32)

            def upright(row):
                return jnp.sum(jnp.where(eye, meta[source, h, pl.ds(row, 1), :], 0.0), axis=1, keepdims=True)

            for k, expert in enumerate((here, there)):
                spread[t, h, k] = (upright(expert) == lane).astype(jnp.bfloat16)
                shares[t, h, k] = jnp.broadcast_to(upright(experts + expert), (tok_count, 128))

        def merge(t, h, i):
            source = order[t]
            back_copy(source, h, i).wait_recv()
            total = None
            for k, block in enumerate((done[source, h, y, :, cols[i]], back_in[source, h, :, cols[i]])):
                scale = jnp.concatenate([shares[t, h, k]] * (step_cols // 128), axis=1)
                term = scale * jnp.dot(spread[t, h, k], block, preferred_element_type=jnp.float32)
                total = term if total is None else total + term
            for way in comes[t]:
                side, arrival = ret_arrival(source, h, i, way)
                arrival.wait_recv()
                total = total + ret_in[side, source, h, :, cols[i]].astype(jnp.float32)
            if t:
                ret_out[source, h, :, cols[i]] = total.astype(jnp.bfloat16)
                ret_copy(source, h, i, leaves[t]).start()
            else:
                last[h, :, cols[i]] = total.astype(jnp.bfloat16)
                pl.when(core != h)(lambda: last_copy(h, i).start())

        def near(t, h, i):
            hop(z, h, i, 0 if at_end else 1).start()

        def far(t, h, i):
            hop(z, h, i, 0).start()

        def own_back(t, h, i):
            back_copy(z, h, i).start()

        def settle():
            for t in range(LINE):
                source = order[t]
                for h in range(2):
                    for way in passes[t]:
                        hop(source, h, None, way).wait_send()
                    cross_copy(source, h, None).wait_send()
                    pair_move(source, h, core, whole).wait_send()
                    part_copy(source, h, None).wait_send()
                    back_copy(source, h, None).wait_send()

        stages = (send_rows, share_rows, up, out, add, turn_over, merge, near, far, own_back)
        for place, number in enumerate(plan):
            if place == len(plan) - SETTLE:
                settle()
            stages[number // 1000](number // 100 % 10, number // 10 % 10, number % 10)
        for t in range(1, LINE):
            for h in range(2):
                ret_copy(order[t], h, None, leaves[t]).wait_send()

    for k in range(len(peers)):
        meta_copy(k).start()
    mate_copy.wait_recv()
    meta_arrival(z, 1 - core).wait_recv()
    pl.when(outer)(lambda: run(OUTER_PLAN, OUTER_TURNS, True))
    pl.when(jnp.logical_not(outer))(lambda: run(INNER_PLAN, INNER_TURNS, False))
    out_ref[:, mine] = last[core]
    for i in range(PARTS):
        last_copy(1 - core, i).wait_recv()
    out_ref[:, other] = last_in[...]
    mate_copy.wait_send()
    for k in range(len(peers)):
        meta_copy(k).wait_send()
    for i in range(PARTS):
        last_copy(1 - core, i).wait_send()


def fused(tokens, norm_gain, expert_ids, route_weights, gate_proj, linear_proj, down_proj):
    tok_count, width = tokens.shape
    picks = expert_ids.shape[1]
    experts = 2 * LINE
    capacity = 2 * tok_count * picks // experts
    ff = gate_proj.shape[2]
    wide, dma = jnp.bfloat16, pltpu.SemaphoreType.DMA
    inside, outside = pl.BlockSpec(memory_space=pltpu.VMEM), pl.BlockSpec(memory_space=pl.ANY)
    return pl.pallas_call(
        kernel,
        out_shape=jax.ShapeDtypeStruct((tok_count, width), wide),
        in_specs=[outside] * 7,
        out_specs=inside,
        scratch_shapes=[
            pltpu.VMEM((picks, tok_count), jnp.int32),
            pltpu.VMEM((picks, tok_count), jnp.float32),
            pltpu.VMEM((1, width), jnp.float32),
            pltpu.VMEM((tok_count, width), wide),
            pltpu.VMEM((width, ff), wide),
            pltpu.VMEM((width, ff), wide),
            pltpu.VMEM((ff, width), wide),
            pltpu.VMEM((tok_count, width // 2), wide),
            pltpu.VMEM((LINE, 2, tok_count, width // 2), wide),
            pltpu.VMEM((LINE, 2, 2 * experts, tok_count), jnp.float32),
            pltpu.VMEM((LINE, 2, 2 * capacity, tok_count), wide),
            pltpu.VMEM((LINE, 2, 2, tok_count, capacity), wide),
            pltpu.VMEM((LINE, 2, 2, tok_count, 128), jnp.float32),
            pltpu.VMEM((LINE, 2, 2, 2, capacity, width // 2), wide),
            pltpu.VMEM((LINE, 2, capacity, width // 2), wide),
            pltpu.VMEM((LINE, 2, 2 * capacity, ff), wide),
            pltpu.VMEM((LINE, 2, 2, 2, capacity, width // 2), wide),
            pltpu.VMEM((LINE, 2, 2, capacity, width // 2), wide),
            pltpu.VMEM((LINE, 2, 2, capacity, width // 2), wide),
            pltpu.VMEM((LINE, 2, capacity, width // 2), wide),
            pltpu.VMEM((2, LINE, 2, tok_count, width // 2), wide),
            pltpu.VMEM((LINE, 2, tok_count, width // 2), wide),
            pltpu.VMEM((2, tok_count, width // 2), wide),
            pltpu.VMEM((tok_count, width // 2), wide),
            dma((7,)),
            dma((1,)), dma((1,)),
            dma((LINE, 2, 2)), dma((LINE, 2, PARTS)),
            dma((2 * LINE - 1,)), dma((LINE, 2)),
            dma((LINE, 2)), dma((LINE, 2, PARTS)),
            dma((LINE, 2)), dma((LINE, 2)),
            dma((LINE, 2)), dma((LINE, 2, BANDS)),
            dma((LINE, 2)), dma((LINE, 2, PARTS)),
            dma((LINE, 2)), dma((2, LINE, 2, PARTS)),
            dma((PARTS,)), dma((PARTS,)),
        ],
        compiler_params=pltpu.CompilerParams(
            collective_id=0, has_side_effects=True, vmem_limit_bytes=60 * 1024 * 1024
        ),
        name="experts",
    )(
        expert_ids.T, route_weights.T, norm_gain.reshape(1, width), tokens,
        gate_proj[0], linear_proj[0], down_proj[0],
    )


def solution(mesh):
    placed = (
        P(("grp", "ep", "tp"), None),
        P(),
        P(("grp", "ep", "tp"), None),
        P(("grp", "ep", "tp"), None),
        P("ep", None, "tp"),
        P("ep", None, "tp"),
        P("ep", "tp", None),
    )
    along = [device.coords[2] for device in mesh.devices[0, :, 0]]
    planned = along == [index // 2 for index in range(2 * LINE)] and mesh.shape["tp"] == 2
    return jax.shard_map(
        fused if planned else shards,
        mesh=mesh,
        in_specs=placed,
        out_specs=P(("grp", "ep", "tp"), None),
        check_vma=False,
    )
```
